32 devices in a mesh: sp: 16 (over z, y, x), tp: 2 (over core).
Axes of the slice: x: 2, y: 2, z: 4, core: 2. Of those that a mesh axis runs over, the one named last changes fastest.
Arguments:
- stream_in: bfloat16 [2048, 2048], P(('sp', 'tp')), may hold values from -6 to 6
- query_compressed: bfloat16 [2048, 512], P('sp'), may hold values from -6 to 6
- keyvalue_compressed: bfloat16 [2048, 256], P('sp'), may hold values from -6 to 6
- rope_key: bfloat16 [2048, 64], P('sp'), may hold values from -153 to 153
- query_norm_gain: float32 [512], replicated, may hold values from 0.1 to 1.9
- keyvalue_norm_gain: float32 [256], replicated, may hold values from 0.1 to 1.9
- query_up_weight: bfloat16 [512, 3072], replicated, may hold values from -0.625 to 0.625
- keyvalue_up_weight: bfloat16 [256, 4096], replicated, may hold values from -0.375 to 0.375
- out_proj: bfloat16 [2048, 2048], replicated, may hold values from -0.5 to 0.5
- ffn_gain: float32 [2048], replicated, may hold values from 0.1 to 1.9
- expert_ids: int32 [2048, 4], P(('sp', 'tp')), may hold values from 0 to 15, all different within a row; in each aligned block of 64 rows (0 to 63, 64 to 127, ...) at most 32 rows name the same one
- expert_weights: float32 [2048, 4], P(('sp', 'tp')), may hold values from 0.1 to 1
- expert_gate: bfloat16 [16, 2048, 512], P('sp', None, 'tp'), may hold values from -0.125 to 0.125
- expert_up: bfloat16 [16, 2048, 512], P('sp', None, 'tp'), may hold values from -0.125 to 0.125
- expert_down: bfloat16 [16, 512, 2048], P('sp', 'tp'), may hold values from -0.25 to 0.25
- shared_gate: bfloat16 [2048, 512], replicated, may hold values from -0.125 to 0.125
- shared_up: bfloat16 [2048, 512], replicated, may hold values from -0.125 to 0.125
- shared_down: bfloat16 [512, 2048], replicated, may hold values from -0.25 to 0.25
Outputs:
- layer_out: bfloat16 [2048, 2048], P(('sp', 'tp'))
The draws below stay inside these ranges and needn't reach their ends.
Inputs may be any that keep to these rules, and one draw needn't show every extreme that they name: `expert_ids`: each row names 4 different experts. Among the rows of one device (aligned blocks of 64 rows in token order) no expert is named by more than 32 rows, a bound that some block reaches of some device.
All inputs are finite; a program needn't handle non-finite values.
Results may differ from the reference program's by a relative error of at most 0.02.
The reference program's roundings to bfloat16 on the way count: a program that leaves them out, or rounds other values in their place, can miss the bound.
Values may be sent and summed in bfloat16 or wider, within the bound.
A program may use at most 128 MiB of HBM per device.

```python
import math
import jax
import jax.numpy as jnp
import numpy as np
from jax import lax

D = 2048
ATTENTION_HEADS = 16
QUERY_RANK = 512
KEYVALUE_RANK = 256
KEY_PLAIN_WIDTH = 128
ROTARY_WIDTH = 64
VALUE_HEAD_WIDTH = 128
FE = 512
FS = 512
TOP = 4
EXPERTS = 16
SEQUENCE_TOKENS = 2048
TOK_MOE = 64
CAP = 32
N_SP = 16


def draw_rope_key(key, part):
    first_key, second_key = jax.random.split(key, 2)
    normal_values = jax.random.normal(first_key, (SEQUENCE_TOKENS, ROTARY_WIDTH), jnp.float32)
    return jnp.clip(normal_values, -4.0, 4.0).astype(jnp.bfloat16)


def shard_levels(own_key, extent, cuts, least, top_value):
    level = 1.0
    for axis_at, blocks in cuts:
        steps = jax.random.uniform(jax.random.fold_in(jax.random.fold_in(own_key, 6), axis_at), (blocks,), jnp.float32, least / len(cuts), top_value / len(cuts))
        level = level * jnp.repeat(jnp.exp(steps), extent[axis_at] // blocks).reshape((-1,) + (1,) * (len(extent) - 1 - axis_at))
    return level


def assign_block(own_key, own, number, rows, amount, top, limit, lean):
    ranking = jax.random.permutation(own_key, amount)
    packed, ordinary = load_shares(amount, rows * top, limit, lean, True), load_shares(amount, rows * top, limit, lean, False)
    places = jnp.arange(amount)

    def named(sizes, turn):
        used = int((sizes > 0).sum())
        fixed = max(1, used // 4)
        passed = fixed + (places - fixed + turn * (used - fixed)) % max(1, amount - fixed)
        return jnp.zeros((amount,), jnp.int32).at[ranking[jnp.where(places < fixed, places, passed)]].set(jnp.asarray(sizes, jnp.int32))

    sizes = jnp.where(number % 4 == 0, named(packed, number // 4), named(ordinary, number - number // 4 - 1))
    mixed = jax.random.permutation(jax.random.fold_in(own, 3), amount)
    source_of, sink = mixed[0:amount // 2 * 2:2], mixed[1:amount // 2 * 2:2]
    room = jnp.minimum(sizes[source_of] - 1, limit - sizes[sink]) // 2
    room = jnp.where((source_of == ranking[0]) | (sink == ranking[0]) | (sizes[sink] == 0), 0, jnp.maximum(room, 0))
    passed = jax.random.randint(jax.random.fold_in(own, 4), (amount // 2,), 0, 1 << 20) % (room + 1)
    sizes = sizes.at[source_of].add(-passed).at[sink].add(passed)
    labels = jnp.searchsorted(jnp.cumsum(sizes), jnp.arange(rows * top), side="right").astype(jnp.int32)
    table = labels.reshape(top, rows).T
    table = table[jax.random.permutation(jax.random.fold_in(own, 1), rows)]
    turn = jax.random.randint(jax.random.fold_in(own, 2), (rows, 1), 0, top)
    return jnp.take_along_axis(table, (jnp.arange(top)[None, :] + turn) % top, axis=1)


def load_shares(number_of, total, most, skew, full):
    portions = [(1 << 20) // math.isqrt(rank ** skew) + 1 for rank in range(1, number_of + 1)]
    largest = most if full else min(most, max(-(-total // number_of), total * portions[0] // sum(portions)))
    least = 1 if total - largest >= number_of - 1 else 0
    holding, surplus = [largest] + [least] * (number_of - 1), total - largest - least * (number_of - 1)
    while surplus > 0:
        candidates = [i for i in range(1, number_of) if holding[i] < largest] or [i for i in range(1, number_of) if holding[i] < most]
        whole, remaining = sum([portions[i] for i in candidates]), surplus
        for i in candidates:
            extra = min(most - holding[i], max(1, remaining * portions[i] // whole), surplus)
            holding[i] = holding[i] + extra
            surplus = surplus - extra
    return np.array(holding)


def bell_draw(rng, dims, scale, bound, pieces=(), kind=jnp.bfloat16):
    array = jax.random.normal(rng, dims, jnp.float32) * scale
    if len(pieces) > 0:
        array = shard_levels(rng, dims, pieces, -0.22, 0.18) * array
    return jnp.clip(array, min=-bound, max=bound).astype(kind)


def setup_inputs(seed: int = 0) -> dict:
    splits = jax.random.split(jax.random.key(seed), 19)
    stream_in = bell_draw(splits[0], (SEQUENCE_TOKENS, D), 1.0, 6.0, ((0, 32),))
    query_compressed = bell_draw(splits[1], (SEQUENCE_TOKENS, QUERY_RANK), 1.0, 6.0, ((0, 16),))
    keyvalue_compressed = bell_draw(splits[2], (SEQUENCE_TOKENS, KEYVALUE_RANK), 1.0, 6.0, ((0, 16),))
    rope_key = draw_rope_key(jax.random.fold_in(splits[18], 71), 0)
    query_norm_gain = jnp.clip(1.0 + 0.18 * jax.random.normal(splits[4], (QUERY_RANK,), jnp.float32), 0.1, 1.9)
    keyvalue_norm_gain = jnp.clip(1.0 + 0.18 * jax.random.normal(splits[5], (KEYVALUE_RANK,), jnp.float32), 0.1, 1.9)
    query_up_weight = bell_draw(splits[6], (QUERY_RANK, ATTENTION_HEADS * (KEY_PLAIN_WIDTH + ROTARY_WIDTH)), (QUERY_RANK // 6) ** -0.5, 0.625)
    keyvalue_up_weight = bell_draw(splits[7], (KEYVALUE_RANK, ATTENTION_HEADS * (KEY_PLAIN_WIDTH + VALUE_HEAD_WIDTH)), KEYVALUE_RANK ** -0.5, 0.375)
    out_proj = bell_draw(splits[8], (ATTENTION_HEADS * VALUE_HEAD_WIDTH, D), (ATTENTION_HEADS * VALUE_HEAD_WIDTH // 16) ** -0.5, 0.5)
    ffn_gain = jnp.clip(1.0 + 0.18 * jax.random.normal(splits[9], (D,), jnp.float32), 0.1, 1.9)
    expert_ids_keys = jax.random.split(jax.random.fold_in(splits[10], 1), SEQUENCE_TOKENS // TOK_MOE)
    expert_ids_turns = jax.random.permutation(jax.random.fold_in(splits[10], 3), SEQUENCE_TOKENS // TOK_MOE)
    expert_ids = jax.vmap(lambda own, number: assign_block(jax.random.fold_in(splits[10], 2), own, number, TOK_MOE, EXPERTS, TOP, CAP, 2))(expert_ids_keys, expert_ids_turns).reshape((SEQUENCE_TOKENS, TOP))
    expert_weights = jnp.clip(0.1 + 0.9 * jax.random.uniform(splits[11], (SEQUENCE_TOKENS, TOP), jnp.float32) ** shard_levels(splits[11], (SEQUENCE_TOKENS, TOP), ((0, 32),), -0.2, 0.2), 0.1, 1.0)
    expert_gate = bell_draw(splits[12], (EXPERTS, D, FE), D ** -0.5, 0.125, ((0, 16), (2, 2)))
    expert_up = bell_draw(splits[13], (EXPERTS, D, FE), D ** -0.5, 0.125, ((0, 16), (2, 2)))
    expert_down = bell_draw(splits[14], (EXPERTS, FE, D), FE ** -0.5, 0.25, ((0, 16), (1, 2)))
    shared_gate = bell_draw(splits[15], (D, FS), D ** -0.5, 0.125)
    shared_up = bell_draw(splits[16], (D, FS), D ** -0.5, 0.125)
    shared_down = bell_draw(splits[17], (FS, D), FS ** -0.5, 0.25)
    return {"stream_in": stream_in, "query_compressed": query_compressed, "keyvalue_compressed": keyvalue_compressed, "rope_key": rope_key, "query_norm_gain": query_norm_gain, "keyvalue_norm_gain": keyvalue_norm_gain, "query_up_weight": query_up_weight, "keyvalue_up_weight": keyvalue_up_weight, "out_proj": out_proj, "ffn_gain": ffn_gain, "expert_ids": expert_ids, "expert_weights": expert_weights, "expert_gate": expert_gate, "expert_up": expert_up, "expert_down": expert_down, "shared_gate": shared_gate, "shared_up": shared_up, "shared_down": shared_down}


epsilon = 1e-06
routed_scale = 2.5
theta_base = 10000.0

def rms_scale(values, scales):
    widened = values.astype(jnp.float32)
    inverse = lax.rsqrt(lax.optimization_barrier(jnp.mean(widened * widened, axis=-1, keepdims=True)) + epsilon)
    return widened * inverse * scales.astype(jnp.float32)

def turn_tables(positions, rot_width):
    half_width = rot_width // 2
    frequency = theta_base ** (-(jnp.arange(half_width, dtype=jnp.float32) * 2.0) / rot_width)
    angles = positions.astype(jnp.float32)[:, None] * frequency[None, :]
    return (jnp.cos(angles), jnp.sin(angles))

def turn(values, cos_part, sine_part):
    lower_half, upper_half = jnp.split(values, 2, axis=-1)
    return jnp.concatenate([lower_half * cos_part - upper_half * sine_part, upper_half * cos_part + lower_half * sine_part], axis=-1)

def reference(stream_in, query_compressed, keyvalue_compressed, rope_key, query_norm_gain, keyvalue_norm_gain, query_up_weight, keyvalue_up_weight, out_proj, ffn_gain, expert_ids, expert_weights, expert_gate, expert_up, expert_down, shared_gate, shared_up, shared_down):
    head_width = KEY_PLAIN_WIDTH + ROTARY_WIDTH
    positions = jnp.arange(SEQUENCE_TOKENS, dtype=jnp.int32)
    cos_part, sine_part = turn_tables(positions, ROTARY_WIDTH)
    query_normed = rms_scale(query_compressed, query_norm_gain).astype(jnp.bfloat16)
    queries = jnp.dot(query_normed, query_up_weight, preferred_element_type=jnp.float32) * head_width ** (-0.5)
    queries = queries.reshape(SEQUENCE_TOKENS, ATTENTION_HEADS, head_width)
    turned = turn(queries[:, :, KEY_PLAIN_WIDTH:], cos_part[:, None, :], sine_part[:, None, :])
    queries = jnp.concatenate([queries[:, :, :KEY_PLAIN_WIDTH], turned], axis=-1).astype(jnp.bfloat16)
    keyval_normed = rms_scale(keyvalue_compressed, keyvalue_norm_gain).astype(jnp.bfloat16)
    keyvals = jnp.dot(keyval_normed, keyvalue_up_weight, preferred_element_type=jnp.float32).astype(jnp.bfloat16)
    keyvals = keyvals.reshape(SEQUENCE_TOKENS, ATTENTION_HEADS, KEY_PLAIN_WIDTH + VALUE_HEAD_WIDTH)
    key_part = keyvals[:, :, :KEY_PLAIN_WIDTH].astype(jnp.float32)
    value_part = keyvals[:, :, KEY_PLAIN_WIDTH:].astype(jnp.float32)
    shared_rot = lax.optimization_barrier(turn(rope_key.astype(jnp.float32), cos_part, sine_part).astype(jnp.bfloat16)).astype(jnp.float32)

    def attend(query_block):
        scores = jnp.einsum('qhd,khd->hqk', query_block[:, :, :KEY_PLAIN_WIDTH], key_part)
        scores = scores + jnp.einsum('qhr,kr->hqk', query_block[:, :, KEY_PLAIN_WIDTH:], shared_rot)
        row_max = lax.optimization_barrier(jnp.max(scores, axis=-1, keepdims=True))
        weights = jnp.exp(scores - row_max)
        row_sum = lax.optimization_barrier(jnp.sum(weights, axis=-1))
        rounded = lax.optimization_barrier(weights.astype(jnp.bfloat16)).astype(jnp.float32)
        summed = jnp.einsum('hqk,khd->qhd', rounded, value_part)
        return (summed / jnp.transpose(row_sum)[:, :, None]).astype(jnp.bfloat16)
    query_blocks = queries.astype(jnp.float32).reshape(SEQUENCE_TOKENS // 64, 64, ATTENTION_HEADS, head_width)
    attended = lax.map(attend, query_blocks).reshape(SEQUENCE_TOKENS, ATTENTION_HEADS * VALUE_HEAD_WIDTH)
    projected = jnp.dot(attended, out_proj, preferred_element_type=jnp.float32)
    stream = (stream_in.astype(jnp.float32) + projected).astype(jnp.bfloat16)
    normed = rms_scale(stream, ffn_gain).astype(jnp.bfloat16)
    shares = (routed_scale * expert_weights / lax.optimization_barrier(jnp.sum(expert_weights, axis=-1, keepdims=True))).astype(jnp.bfloat16)
    flat_ids = expert_ids.reshape(-1)
    assign_count = flat_ids.shape[0]
    flat_shares = jnp.concatenate([shares.reshape(-1), jnp.zeros((1,), jnp.bfloat16)])
    padded = jnp.concatenate([normed, jnp.zeros((1, D), jnp.bfloat16)], axis=0)
    slot_count = 2 * N_SP * CAP
    half_hidden = FE // 2

    def run_expert(accumulated, expert):
        picked = jnp.nonzero(flat_ids == expert, size=slot_count, fill_value=assign_count)[0].astype(jnp.int32)
        row_ids = (picked // TOP).astype(jnp.int32)
        inputs = padded[row_ids]
        gate_act = jnp.dot(inputs, expert_gate[expert], preferred_element_type=jnp.float32)
        up_act = jnp.dot(inputs, expert_up[expert], preferred_element_type=jnp.float32)
        inner_act = (jax.nn.silu(gate_act) * up_act).astype(jnp.bfloat16)
        down_rows = expert_down[expert]
        first_half = jnp.dot(inner_act[:, :half_hidden], down_rows[:half_hidden], preferred_element_type=jnp.float32).astype(jnp.bfloat16)
        second_half = jnp.dot(inner_act[:, half_hidden:], down_rows[half_hidden:], preferred_element_type=jnp.float32).astype(jnp.bfloat16)
        output = (first_half.astype(jnp.float32) + second_half.astype(jnp.float32)).astype(jnp.bfloat16)
        weighted = output.astype(jnp.float32) * flat_shares[picked].astype(jnp.float32)[:, None]
        return (accumulated.at[row_ids].add(weighted), None)
    routed, _ = lax.scan(run_expert, jnp.zeros((SEQUENCE_TOKENS + 1, D), jnp.float32), jnp.arange(EXPERTS, dtype=jnp.int32))
    shared_inner = (jax.nn.silu(jnp.dot(normed, shared_gate, preferred_element_type=jnp.float32)) * jnp.dot(normed, shared_up, preferred_element_type=jnp.float32)).astype(jnp.bfloat16)
    shared_out = jnp.dot(shared_inner, shared_down, preferred_element_type=jnp.float32)
    return (stream.astype(jnp.float32) + routed[:SEQUENCE_TOKENS] + shared_out).astype(jnp.bfloat16)
```

```python
import functools

import jax
import jax.numpy as jnp
from jax import lax
from jax.experimental import pallas as pl
from jax.experimental.pallas import tpu as pltpu
from jax.sharding import PartitionSpec as P

KEY_PLAIN_WIDTH = 128
ROTARY_WIDTH = 64
VALUE_HEAD_WIDTH = 128
LANES = 128

epsilon = 1e-06
routed_scale = 2.5
theta_base = 10000.0
MESH = pl.DeviceIdType.MESH
F32 = jnp.float32
BF16 = jnp.bfloat16


def rms_scale(values, scales):
    widened = values.astype(F32)
    inverse = lax.rsqrt(jnp.mean(widened * widened, axis=-1, keepdims=True) + epsilon)
    return widened * inverse * scales


def turn_tables(positions, rot_width):
    half_width = rot_width // 2
    frequency = theta_base ** (-(jnp.arange(half_width, dtype=F32) * 2.0) / rot_width)
    angles = positions.astype(F32)[:, None] * frequency[None, :]
    return (jnp.cos(angles), jnp.sin(angles))


def turn(values, cos_part, sine_part):
    lower_half, upper_half = jnp.split(values, 2, axis=-1)
    return jnp.concatenate(
        [
            lower_half * cos_part - upper_half * sine_part,
            upper_half * cos_part + lower_half * sine_part,
        ],
        axis=-1,
    )


def line_length(n):
    for candidate in (4, 2):
        if n % candidate == 0:
            return candidate
    return 1


def remote(src, dst, send_sem, recv_sem, sp, tp):
    return pltpu.make_async_remote_copy(
        src_ref=src,
        dst_ref=dst,
        send_sem=send_sem,
        recv_sem=recv_sem,
        device_id=(sp, tp),
        device_id_type=MESH,
    )


def greet(n, nz, with_partner):
    pn = n // nz
    me, t = lax.axis_index("sp"), lax.axis_index("tp")
    z, p = me // pn, me % pn
    barrier = pltpu.get_barrier_semaphore()
    for dz in range(1, nz):
        pl.semaphore_signal(
            barrier, inc=1, device_id=(((z + dz) % nz) * pn + p, t), device_id_type=MESH
        )
    for d in range(1, pn):
        pl.semaphore_signal(
            barrier, inc=1, device_id=(z * pn + (p + d) % pn, t), device_id_type=MESH
        )
    if with_partner:
        pl.semaphore_signal(barrier, inc=1, device_id=(me, 1 - t), device_id_type=MESH)
    pl.semaphore_wait(barrier, nz - 1 + pn - 1 + (1 if with_partner else 0))


def gather_kernel(
    n, nz, x_ref, g_ref, u_ref, d_ref, kv_ref, go_ref, uo_ref, do_ref,
    zs, zr, ps, pr, xs, xr, ws, wr,
):
    pn = n // nz
    me, t = lax.axis_index("sp"), lax.axis_index("tp")
    z, p = me // pn, me % pn
    greet(n, nz, True)

    def block_of(dz, d):
        return ((z - dz + nz) % nz) * pn + (p - d + pn) % pn

    def along(dz):
        return remote(
            x_ref.at[t], kv_ref.at[me, t], zs.at[dz], zr.at[dz], ((z + dz) % nz) * pn + p, t
        )

    def across(dz, d):
        b = block_of(dz, 0)
        src = x_ref.at[t] if dz == 0 else kv_ref.at[b, t]
        return remote(
            src, kv_ref.at[b, t], ps.at[dz, d], pr.at[dz, d], z * pn + (p + d) % pn, t
        )

    def swap(dz, d):
        b = block_of(dz, d)
        return remote(
            kv_ref.at[b, t], kv_ref.at[b, t], xs.at[dz, d], xr.at[dz, d], me, 1 - t
        )

    weights = [
        remote(g_ref, go_ref, ws.at[0], wr.at[0], me, 1 - t),
        remote(u_ref, uo_ref, ws.at[1], wr.at[1], me, 1 - t),
        remote(d_ref, do_ref, ws.at[2], wr.at[2], me, 1 - t),
    ]
    for dz in range(1, nz):
        along(dz).start()
    for d in range(1, pn):
        across(0, d).start()
    for copy in weights:
        copy.start()
    kv_ref[me] = x_ref[...]
    for dz in range(1, nz):
        along(dz).wait_recv()
        for d in range(1, pn):
            across(dz, d).start()
        swap(dz, 0).start()
    for dz in range(nz):
        for d in range(1, pn):
            across(dz, d).wait_recv()
            swap(dz, d).start()
    for dz in range(nz):
        for d in range(pn):
            if dz or d:
                swap(dz, d).wait()
    for dz in range(1, nz):
        along(dz).wait_send()
    for dz in range(nz):
        for d in range(1, pn):
            across(dz, d).wait_send()
    for copy in weights:
        copy.wait()


def gather_latents(n, nz, packed, gate, up, down):
    pn = n // nz
    rows, width = packed.shape
    anywhere = pl.BlockSpec(memory_space=pl.ANY)
    inside = pl.BlockSpec(memory_space=pltpu.VMEM)
    return pl.pallas_call(
        functools.partial(gather_kernel, n, nz),
        out_shape=(
            jax.ShapeDtypeStruct((n, 2, rows // 2, width), BF16),
            jax.ShapeDtypeStruct(gate.shape, BF16),
            jax.ShapeDtypeStruct(up.shape, BF16),
            jax.ShapeDtypeStruct(down.shape, BF16),
        ),
        in_specs=[inside, anywhere, anywhere, anywhere],
        out_specs=(inside, anywhere, anywhere, anywhere),
        scratch_shapes=[
            pltpu.SemaphoreType.DMA((nz,)),
            pltpu.SemaphoreType.DMA((nz,)),
            pltpu.SemaphoreType.DMA((nz, pn)),
            pltpu.SemaphoreType.DMA((nz, pn)),
            pltpu.SemaphoreType.DMA((nz, pn)),
            pltpu.SemaphoreType.DMA((nz, pn)),
            pltpu.SemaphoreType.DMA((3,)),
            pltpu.SemaphoreType.DMA((3,)),
        ],
        compiler_params=pltpu.CompilerParams(collective_id=0, has_side_effects=True),
        name="gather_latents",
    )(packed.reshape(2, rows // 2, width), gate, up, down)


NT = (((1,), (1,)), ((), ()))
TN = (((0,), (0,)), ((), ()))


def attend_kernel(heads, t_ref, qn_ref, qr_ref, w_ref, kv_ref, out_ref):
    latent = kv_ref.shape[1] - LANES
    pair = KEY_PLAIN_WIDTH + VALUE_HEAD_WIDTH
    rows = qn_ref.shape[1]
    parts = []
    for h in range(heads):
        wk = w_ref[:, h * pair : h * pair + KEY_PLAIN_WIDTH]
        qa = lax.dot_general(qn_ref[h], wk, NT, preferred_element_type=F32).astype(BF16)
        parts.append(jnp.concatenate([qa, qr_ref[h]], axis=1))
    q = jnp.concatenate(parts, axis=0)
    scores = lax.dot_general(q, kv_ref[...], NT, preferred_element_type=F32)
    weights = jnp.exp(scores - jnp.max(scores, axis=-1, keepdims=True))
    total = jnp.sum(weights, axis=-1, keepdims=True)
    mixed = jnp.dot(weights.astype(BF16), kv_ref[:, :latent], preferred_element_type=F32)
    mixed = (mixed / total).astype(BF16)
    for h in range(heads):
        wv = w_ref[:, h * pair + KEY_PLAIN_WIDTH : (h + 1) * pair]
        out_ref[:, h * VALUE_HEAD_WIDTH : (h + 1) * VALUE_HEAD_WIDTH] = jnp.dot(
            mixed[h * rows : (h + 1) * rows], wv, preferred_element_type=F32
        ).astype(BF16)


def attend(tp_index, plain, rotary, weight, kv, heads):
    local_heads, rows, _ = plain.shape
    steps = local_heads // heads
    pair = KEY_PLAIN_WIDTH + VALUE_HEAD_WIDTH
    return pl.pallas_call(
        functools.partial(attend_kernel, heads),
        grid_spec=pltpu.PrefetchScalarGridSpec(
            num_scalar_prefetch=1,
            grid=(steps,),
            in_specs=[
                pl.BlockSpec((heads, rows, LANES), lambda i, t: (i, 0, 0)),
                pl.BlockSpec((heads, rows, LANES), lambda i, t: (i, 0, 0)),
                pl.BlockSpec((weight.shape[0], heads * pair), lambda i, t: (0, t[0] * steps + i)),
                pl.BlockSpec(kv.shape, lambda i, t: (0, 0)),
            ],
            out_specs=pl.BlockSpec((rows, heads * VALUE_HEAD_WIDTH), lambda i, t: (0, i)),
        ),
        out_shape=jax.ShapeDtypeStruct((rows, local_heads * VALUE_HEAD_WIDTH), BF16),
        compiler_params=pltpu.CompilerParams(vmem_limit_bytes=60 * 1024 * 1024),
        name="attend",
    )(tp_index.reshape(1), plain, rotary, weight, kv)


def silu(v):
    return v / (1.0 + jnp.exp(-v))


def moe_kernel(
    n, nz, cap,
    normed_ref, stream_ref, maps_ref, g_ref, u_ref, d_ref, go_ref, uo_ref, do_ref,
    sg_ref, su_ref, sd_ref, out_ref,
    wg, wu, wd, sg, su, sd, zb, zm, sb, ab, ob, rb, pb, qb, acc,
    ls, zs, zr, ms, mr, ps, pr, rs, rr, cs, cr,
):
    pn = n // nz
    slots = pn * cap
    width = normed_ref.shape[1]
    me, t = lax.axis_index("sp"), lax.axis_index("tp")
    z, p = me // pn, me % pn
    loads = [
        pltpu.make_async_copy(src, dst, ls.at[i])
        for i, (src, dst) in enumerate(
            [
                (g_ref, wg.at[0]), (go_ref, wg.at[1]), (u_ref, wu.at[0]), (uo_ref, wu.at[1]),
                (d_ref, wd.at[0]), (do_ref, wd.at[1]), (sg_ref, sg), (su_ref, su), (sd_ref, sd),
            ]
        )
    ]
    for copy in loads:
        copy.start()
    greet(n, nz, False)

    def ahead(dz):
        return ((z + dz) % nz) * pn + p

    def rows_along(dz):
        return remote(normed_ref, zb.at[dz], zs.at[dz], zr.at[dz], ahead(dz), t)

    def maps_along(dz):
        return remote(
            maps_ref.at[(z + dz) % nz], zm.at[dz], ms.at[dz], mr.at[dz], ahead(dz), t
        )

    def across(dz, d):
        q = (p + d) % pn
        return remote(
            sb.at[dz, q], ab.at[dz, d], ps.at[dz, d], pr.at[dz, d], z * pn + q, t
        )

    def back(dz, d):
        q = (p - d + pn) % pn
        return remote(
            ob.at[dz, d], rb.at[dz, p], rs.at[dz, d], rr.at[dz, d], z * pn + q, t
        )

    def home(dz):
        return remote(
            pb.at[dz], qb.at[dz], cs.at[dz], cr.at[dz], ((z - dz + nz) % nz) * pn + p, t
        )

    for dz in range(1, nz):
        maps_along(dz).start()
        rows_along(dz).start()
    zb[0] = normed_ref[...]
    zm[0] = maps_ref[z]

    def pick(dz, carried):
        @pl.when(dz > 0)
        def _():
            maps_along(dz).wait_recv()
            rows_along(dz).wait_recv()

        chosen = lax.dot_general(
            zm[dz][:, :slots], zb[dz], TN, preferred_element_type=F32
        )
        for q in range(pn):
            sb[dz, q] = chosen[q * cap : (q + 1) * cap].astype(BF16)
        ab[dz, 0] = sb[dz, p]
        for d in range(1, pn):
            across(dz, d).start()
        return carried

    lax.fori_loop(0, nz, pick, 0)
    for copy in loads:
        copy.wait()
    normed = normed_ref[...]
    shared_inner = (
        silu(jnp.dot(normed, sg[...], preferred_element_type=F32))
        * jnp.dot(normed, su[...], preferred_element_type=F32)
    ).astype(BF16)
    acc[...] = stream_ref[...].astype(F32) + jnp.dot(
        shared_inner, sd[...], preferred_element_type=F32
    )

    def stack(ref, dz):
        if cap % 16 == 0:
            return ref[dz].reshape(slots, width)
        return jnp.concatenate([ref[dz, d].astype(F32) for d in range(pn)], axis=0).astype(BF16)

    def expert(dz, carried):
        for d in range(1, pn):
            across(dz, d).wait_recv()
        rows = stack(ab, dz)
        halves = []
        for h in range(2):
            gate_act = jnp.dot(rows, wg[h], preferred_element_type=F32)
            up_act = jnp.dot(rows, wu[h], preferred_element_type=F32)
            inner = (silu(gate_act) * up_act).astype(BF16)
            halves.append(jnp.dot(inner, wd[h], preferred_element_type=F32).astype(BF16))
        summed = halves[0].astype(F32) + halves[1].astype(F32)
        for d in range(pn):
            ob[dz, d] = summed[d * cap : (d + 1) * cap].astype(BF16)
        rb[dz, p] = ob[dz, 0]
        for d in range(1, pn):
            back(dz, d).start()
        return carried

    lax.fori_loop(0, nz, expert, 0)

    def combine(dz, carried):
        for d in range(1, pn):
            back(dz, d).wait_recv()
        part = jnp.dot(zm[dz][:, slots:], stack(rb, dz), preferred_element_type=F32)

        @pl.when(dz == 0)
        def _():
            acc[...] += part

        @pl.when(dz > 0)
        def _():
            pb[dz] = part.astype(BF16)
            home(dz).start()

        return carried

    lax.fori_loop(0, nz, combine, 0)
    total = acc[...]
    for dz in range(1, nz):
        home(dz).wait_recv()
        total = total + qb[dz].astype(F32)
    out_ref[...] = total.astype(BF16)
    for dz in range(1, nz):
        maps_along(dz).wait_send()
        rows_along(dz).wait_send()
        home(dz).wait_send()
    for dz in range(nz):
        for d in range(1, pn):
            across(dz, d).wait_send()
            back(dz, d).wait_send()


def experts(n, nz, cap, normed, stream, maps, weights, shared):
    pn = n // nz
    rows, width = normed.shape
    hidden = weights[0].shape[1]
    shared_hidden = shared[0].shape[1]
    anywhere = pl.BlockSpec(memory_space=pl.ANY)
    inside = pl.BlockSpec(memory_space=pltpu.VMEM)
    plane = (nz, pn, cap, width)
    dma = pltpu.SemaphoreType.DMA
    return pl.pallas_call(
        functools.partial(moe_kernel, n, nz, cap),
        out_shape=jax.ShapeDtypeStruct((rows, width), BF16),
        in_specs=[inside] * 3 + [anywhere] * 9,
        out_specs=inside,
        scratch_shapes=[
            pltpu.VMEM((2, width, hidden), BF16),
            pltpu.VMEM((2, width, hidden), BF16),
            pltpu.VMEM((2, hidden, width), BF16),
            pltpu.VMEM((width, shared_hidden), BF16),
            pltpu.VMEM((width, shared_hidden), BF16),
            pltpu.VMEM((shared_hidden, width), BF16),
            pltpu.VMEM((nz, rows, width), BF16),
            pltpu.VMEM((nz, rows, maps.shape[2]), BF16),
            pltpu.VMEM(plane, BF16),
            pltpu.VMEM(plane, BF16),
            pltpu.VMEM(plane, BF16),
            pltpu.VMEM(plane, BF16),
            pltpu.VMEM((nz, rows, width), BF16),
            pltpu.VMEM((nz, rows, width), BF16),
            pltpu.VMEM((rows, width), F32),
            dma((9,)),
            dma((nz,)), dma((nz,)), dma((nz,)), dma((nz,)),
            dma((nz, pn)), dma((nz, pn)), dma((nz, pn)), dma((nz, pn)),
            dma((nz,)), dma((nz,)),
        ],
        compiler_params=pltpu.CompilerParams(
            collective_id=1, has_side_effects=True, vmem_limit_bytes=60 * 1024 * 1024
        ),
        name="experts",
    )(normed, stream, maps, *weights, *shared)


def shards(
    n,
    stream_in,
    query_compressed,
    keyvalue_compressed,
    rope_key,
    query_norm_gain,
    keyvalue_norm_gain,
    query_up_weight,
    keyvalue_up_weight,
    out_proj,
    ffn_gain,
    expert_ids,
    expert_weights,
    expert_gate,
    expert_up,
    expert_down,
    shared_gate,
    shared_up,
    shared_down,
):
    nz = line_length(n)
    tok_rows = query_compressed.shape[0]
    head_width = KEY_PLAIN_WIDTH + ROTARY_WIDTH
    all_heads = query_up_weight.shape[1] // head_width
    local_heads = all_heads // 2
    sp_index = lax.axis_index("sp")
    tp_index = lax.axis_index("tp")
    own_pos = sp_index * tok_rows + jnp.arange(tok_rows, dtype=jnp.int32)
    cos_part, sine_part = turn_tables(own_pos, ROTARY_WIDTH)

    keyval_normed = rms_scale(keyvalue_compressed, keyvalue_norm_gain).astype(BF16)
    shared_rot = turn(rope_key.astype(F32), cos_part, sine_part).astype(BF16)
    fill = jnp.zeros((tok_rows, LANES - ROTARY_WIDTH), BF16)
    packed = jnp.concatenate([keyval_normed, shared_rot, fill], axis=1)
    kv, gate_other, up_other, down_other = gather_latents(
        n, nz, packed, expert_gate[0], expert_up[0], expert_down[0]
    )
    kv = kv.reshape(n * tok_rows, packed.shape[1])

    query_normed = rms_scale(query_compressed, query_norm_gain).astype(BF16)
    query_cols = lax.dynamic_slice_in_dim(
        query_up_weight, tp_index * local_heads * head_width, local_heads * head_width, 1
    )
    raw_query = jnp.dot(query_normed, query_cols, preferred_element_type=F32) * head_width ** (-0.5)
    raw_query = raw_query.reshape(tok_rows, local_heads, head_width)
    turned = turn(raw_query[:, :, KEY_PLAIN_WIDTH:], cos_part[:, None, :], sine_part[:, None, :])
    plain = jnp.transpose(raw_query[:, :, :KEY_PLAIN_WIDTH].astype(BF16), (1, 0, 2))
    rotary = jnp.transpose(
        jnp.pad(turned.astype(BF16), ((0, 0), (0, 0), (0, LANES - ROTARY_WIDTH))), (1, 0, 2)
    )
    local_out = attend(tp_index, plain, rotary, keyvalue_up_weight, kv, 2)

    attended = lax.all_to_all(local_out, "tp", split_axis=0, concat_axis=1, tiled=True)
    projected = jnp.dot(attended, out_proj, preferred_element_type=F32)
    stream = (stream_in.astype(F32) + projected).astype(BF16)
    normed = rms_scale(stream, ffn_gain).astype(BF16)

    shares = (
        routed_scale * expert_weights / jnp.sum(expert_weights, axis=-1, keepdims=True)
    ).astype(BF16)
    moe_rows = stream_in.shape[0]
    top_count = expert_ids.shape[1]
    expert_count = expert_gate.shape[0] * n
    capacity = 2 * moe_rows * top_count // expert_count
    slots = expert_count // nz * capacity
    flat_ids = expert_ids.reshape(-1)
    hot_ids = (flat_ids[:, None] == jnp.arange(expert_count, dtype=jnp.int32)[None, :]).astype(
        jnp.int32
    )
    rank_ids = jnp.sum((jnp.cumsum(hot_ids, axis=0) - hot_ids) * hot_ids, axis=1)
    slot_ids = flat_ids * capacity + rank_ids
    hot_slots = (
        slot_ids[:, None] == jnp.arange(expert_count * capacity, dtype=jnp.int32)[None, :]
    ).reshape(moe_rows, top_count, expert_count * capacity)
    sender_map = jnp.any(hot_slots, axis=1).astype(BF16).reshape(moe_rows, nz, slots)
    share_map = jnp.sum(
        jnp.where(hot_slots, shares[:, :, None], jnp.zeros((), BF16)), axis=1
    ).reshape(moe_rows, nz, slots)
    maps = jnp.transpose(jnp.concatenate([sender_map, share_map], axis=2), (1, 0, 2))
    return experts(
        n, nz, capacity, normed, stream, maps,
        (expert_gate[0], expert_up[0], expert_down[0], gate_other, up_other, down_other),
        (shared_gate, shared_up, shared_down),
    )


def solution(mesh):
    in_specs = (
        P(("sp", "tp"), None),
        P("sp", None),
        P("sp", None),
        P("sp", None),
        P(),
        P(),
        P(),
        P(),
        P(),
        P(),
        P(("sp", "tp"), None),
        P(("sp", "tp"), None),
        P("sp", None, "tp"),
        P("sp", None, "tp"),
        P("sp", "tp", None),
        P(),
        P(),
        P(),
    )
    return jax.shard_map(
        functools.partial(shards, mesh.shape["sp"]),
        mesh=mesh,
        in_specs=in_specs,
        out_specs=P(("sp", "tp"), None),
        check_vma=False,
    )
```

```python
import functools

import jax
import jax.numpy as jnp
from jax import lax
from jax.experimental import pallas as pl
from jax.experimental.pallas import tpu as pltpu
from jax.sharding import PartitionSpec as P

KEY_PLAIN_WIDTH = 128
ROTARY_WIDTH = 64
VALUE_HEAD_WIDTH = 128
LANES = 128

epsilon = 1e-06
routed_scale = 2.5
theta_base = 10000.0
MESH = pl.DeviceIdType.MESH
F32 = jnp.float32
BF16 = jnp.bfloat16


def rms_scale(values, scales):
    widened = values.astype(F32)
    inverse = lax.rsqrt(jnp.mean(widened * widened, axis=-1, keepdims=True) + epsilon)
    return widened * inverse * scales


def turn_tables(positions, rot_width):
    half_width = rot_width // 2
    frequency = theta_base ** (-(jnp.arange(half_width, dtype=F32) * 2.0) / rot_width)
    angles = positions.astype(F32)[:, None] * frequency[None, :]
    return (jnp.cos(angles), jnp.sin(angles))


def turn(values, cos_part, sine_part):
    lower_half, upper_half = jnp.split(values, 2, axis=-1)
    return jnp.concatenate(
        [
            lower_half * cos_part - upper_half * sine_part,
            upper_half * cos_part + lower_half * sine_part,
        ],
        axis=-1,
    )


def line_length(n):
    for candidate in (4, 2):
        if n % candidate == 0:
            return candidate
    return 1


def nearest(nz, z, k):
    place = jnp.int32(0)
    for at in range(nz):
        order = sorted(range(nz), key=lambda other: (abs(other - at), other))
        place = place + jnp.where(z == at, order[k], 0)
    return place


def remote(src, dst, send_sem, recv_sem, sp, tp):
    return pltpu.make_async_remote_copy(
        src_ref=src,
        dst_ref=dst,
        send_sem=send_sem,
        recv_sem=recv_sem,
        device_id=(sp, tp),
        device_id_type=MESH,
    )


def greet(n, nz, with_partner):
    pn = n // nz
    me, t = lax.axis_index("sp"), lax.axis_index("tp")
    z, p = me // pn, me % pn
    barrier = pltpu.get_barrier_semaphore()
    for dz in range(1, nz):
        pl.semaphore_signal(
            barrier, inc=1, device_id=(((z + dz) % nz) * pn + p, t), device_id_type=MESH
        )
    for d in range(1, pn):
        pl.semaphore_signal(
            barrier, inc=1, device_id=(z * pn + (p + d) % pn, t), device_id_type=MESH
        )
    if with_partner:
        pl.semaphore_signal(barrier, inc=1, device_id=(me, 1 - t), device_id_type=MESH)
    pl.semaphore_wait(barrier, nz - 1 + pn - 1 + (1 if with_partner else 0))


def gather_kernel(
    n, nz, x_ref, g_ref, u_ref, d_ref, kv_ref, go_ref, uo_ref, do_ref,
    zs, zr, ps, pr, xs, xr, ws, wr,
):
    pn = n // nz
    me, t = lax.axis_index("sp"), lax.axis_index("tp")
    z, p = me // pn, me % pn
    greet(n, nz, True)

    def block_of(dz, d):
        return ((z - dz + nz) % nz) * pn + (p - d + pn) % pn

    def along(dz):
        return remote(
            x_ref.at[t], kv_ref.at[me, t], zs.at[dz], zr.at[dz], ((z + dz) % nz) * pn + p, t
        )

    def across(dz, d):
        b = block_of(dz, 0)
        src = x_ref.at[t] if isinstance(dz, int) else kv_ref.at[b, t]
        return remote(
            src, kv_ref.at[b, t], ps.at[dz, d], pr.at[dz, d], z * pn + (p + d) % pn, t
        )

    def swap(dz, d):
        b = block_of(dz, d)
        return remote(
            kv_ref.at[b, t], kv_ref.at[b, t], xs.at[dz, d], xr.at[dz, d], me, 1 - t
        )

    weights = [
        remote(g_ref, go_ref, ws.at[0], wr.at[0], me, 1 - t),
        remote(u_ref, uo_ref, ws.at[1], wr.at[1], me, 1 - t),
        remote(d_ref, do_ref, ws.at[2], wr.at[2], me, 1 - t),
    ]
    away = [(nearest(nz, z, k) - z + nz) % nz for k in range(nz)]
    for k in range(1, nz):
        along(away[k]).start()
    for d in range(1, pn):
        across(0, d).start()
    for copy in weights:
        copy.start()
    kv_ref[me] = x_ref[...]
    behind = [jnp.int32(0)] + [(z - nearest(nz, z, k) + nz) % nz for k in range(1, nz)]
    for k in range(1, nz):
        dz = behind[k]
        along(dz).wait_recv()
        for d in range(1, pn):
            across(dz, d).start()
        swap(dz, 0).start()
    for k in range(nz):
        for d in range(1, pn):
            across(behind[k], d).wait_recv()
            swap(behind[k], d).start()
    for dz in range(nz):
        for d in range(pn):
            if dz or d:
                swap(dz, d).wait()
    for dz in range(1, nz):
        along(dz).wait_send()
    for dz in range(nz):
        for d in range(1, pn):
            across(dz, d).wait_send()
    for copy in weights:
        copy.wait()


def gather_latents(n, nz, packed, gate, up, down):
    pn = n // nz
    rows, width = packed.shape
    anywhere = pl.BlockSpec(memory_space=pl.ANY)
    inside = pl.BlockSpec(memory_space=pltpu.VMEM)
    return pl.pallas_call(
        functools.partial(gather_kernel, n, nz),
        out_shape=(
            jax.ShapeDtypeStruct((n, 2, rows // 2, width), BF16),
            jax.ShapeDtypeStruct(gate.shape, BF16),
            jax.ShapeDtypeStruct(up.shape, BF16),
            jax.ShapeDtypeStruct(down.shape, BF16),
        ),
        in_specs=[inside, anywhere, anywhere, anywhere],
        out_specs=(inside, anywhere, anywhere, anywhere),
        scratch_shapes=[
            pltpu.SemaphoreType.DMA((nz,)),
            pltpu.SemaphoreType.DMA((nz,)),
            pltpu.SemaphoreType.DMA((nz, pn)),
            pltpu.SemaphoreType.DMA((nz, pn)),
            pltpu.SemaphoreType.DMA((nz, pn)),
            pltpu.SemaphoreType.DMA((nz, pn)),
            pltpu.SemaphoreType.DMA((3,)),
            pltpu.SemaphoreType.DMA((3,)),
        ],
        compiler_params=pltpu.CompilerParams(collective_id=0, has_side_effects=True),
        name="gather_latents",
    )(packed.reshape(2, rows // 2, width), gate, up, down)


NT = (((1,), (1,)), ((), ()))
TN = (((0,), (0,)), ((), ()))


def attend_kernel(heads, t_ref, x_ref, cos_ref, sin_ref, wq_ref, w_ref, kv_ref, out_ref):
    latent = kv_ref.shape[1] - LANES
    pair = KEY_PLAIN_WIDTH + VALUE_HEAD_WIDTH
    rows = x_ref.shape[0]
    scale = (KEY_PLAIN_WIDTH + ROTARY_WIDTH) ** (-0.5)
    raw = jnp.dot(x_ref[...], wq_ref[...], preferred_element_type=F32) * scale
    first, middle, last = raw[:, :LANES], raw[:, LANES : 2 * LANES], raw[:, 2 * LANES :]
    lane = lax.broadcasted_iota(jnp.int32, (rows, LANES), 1)
    low = lane < ROTARY_WIDTH
    middle_swapped = pltpu.roll(middle, LANES - ROTARY_WIDTH, 1)
    last_swapped = pltpu.roll(last, LANES - ROTARY_WIDTH, 1)
    plain = (first, jnp.where(low, middle_swapped, last_swapped))
    half = ROTARY_WIDTH // 2
    parts = []
    for h, rotary in enumerate((middle, last_swapped)):
        other = jnp.where(
            lane < half, pltpu.roll(rotary, LANES - half, 1), pltpu.roll(rotary, half, 1)
        )
        turned = jnp.where(low, rotary * cos_ref[...] + other * sin_ref[...], 0.0).astype(BF16)
        wk = w_ref[:, h * pair : h * pair + KEY_PLAIN_WIDTH]
        qa = lax.dot_general(plain[h].astype(BF16), wk, NT, preferred_element_type=F32)
        parts.append(jnp.concatenate([qa.astype(BF16), turned], axis=1))
    q = jnp.concatenate(parts, axis=0)
    scores = lax.dot_general(q, kv_ref[...], NT, preferred_element_type=F32)
    weights = jnp.exp(scores - jnp.max(scores, axis=-1, keepdims=True))
    total = jnp.sum(weights, axis=-1, keepdims=True)
    mixed = jnp.dot(weights.astype(BF16), kv_ref[:, :latent], preferred_element_type=F32)
    mixed = (mixed / total).astype(BF16)
    for h in range(heads):
        wv = w_ref[:, h * pair + KEY_PLAIN_WIDTH : (h + 1) * pair]
        out_ref[:, h * VALUE_HEAD_WIDTH : (h + 1) * VALUE_HEAD_WIDTH] = jnp.dot(
            mixed[h * rows : (h + 1) * rows], wv, preferred_element_type=F32
        ).astype(BF16)


def attend(tp_index, query, cos_table, sin_table, query_weight, weight, kv, local_heads):
    heads = 2
    rows, rank = query.shape
    steps = local_heads // heads
    pair = KEY_PLAIN_WIDTH + VALUE_HEAD_WIDTH
    query_block = heads * (KEY_PLAIN_WIDTH + ROTARY_WIDTH)
    return pl.pallas_call(
        functools.partial(attend_kernel, heads),
        grid_spec=pltpu.PrefetchScalarGridSpec(
            num_scalar_prefetch=1,
            grid=(steps,),
            in_specs=[
                pl.BlockSpec((rows, rank), lambda i, t: (0, 0)),
                pl.BlockSpec((rows, LANES), lambda i, t: (0, 0)),
                pl.BlockSpec((rows, LANES), lambda i, t: (0, 0)),
                pl.BlockSpec((rank, query_block), lambda i, t: (0, t[0] * steps + i)),
                pl.BlockSpec((weight.shape[0], heads * pair), lambda i, t: (0, t[0] * steps + i)),
                pl.BlockSpec(kv.shape, lambda i, t: (0, 0)),
            ],
            out_specs=pl.BlockSpec((rows, heads * VALUE_HEAD_WIDTH), lambda i, t: (0, i)),
        ),
        out_shape=jax.ShapeDtypeStruct((rows, local_heads * VALUE_HEAD_WIDTH), BF16),
        compiler_params=pltpu.CompilerParams(vmem_limit_bytes=60 * 1024 * 1024),
        name="attend",
    )(tp_index.reshape(1), query, cos_table, sin_table, query_weight, weight, kv)


def silu(v):
    return v / (1.0 + jnp.exp(-v))


def moe_kernel(
    n, nz, cap,
    normed_ref, stream_ref, maps_ref, g_ref, u_ref, d_ref, go_ref, uo_ref, do_ref,
    sg_ref, su_ref, sd_ref, out_ref,
    wg, wu, wd, sg, su, sd, zb, zm, sb, ab, ob, rb, pb, qb, acc,
    ls, zs, zr, ms, mr, ps, pr, rs, rr, cs, cr,
):
    pn = n // nz
    slots = pn * cap
    width = normed_ref.shape[1]
    me, t = lax.axis_index("sp"), lax.axis_index("tp")
    z, p = me // pn, me % pn
    loads = [
        pltpu.make_async_copy(src, dst, ls.at[i])
        for i, (src, dst) in enumerate(
            [
                (g_ref, wg.at[0]), (go_ref, wg.at[1]), (u_ref, wu.at[0]), (uo_ref, wu.at[1]),
                (d_ref, wd.at[0]), (do_ref, wd.at[1]), (sg_ref, sg), (su_ref, su), (sd_ref, sd),
            ]
        )
    ]
    for copy in loads:
        copy.start()
    greet(n, nz, False)

    near = [nearest(nz, z, k) for k in range(nz)]

    def hop(src, b, step):
        return remote(
            src, zb.at[b], zs.at[b, (step + 1) // 2], zr.at[b], (z + step) * pn + p, t
        )

    def maps_along(dz):
        to = (z + dz) % nz
        return remote(maps_ref.at[to], zm.at[z], ms.at[to], mr.at[z], to * pn + p, t)

    def across(b, d):
        q = (p + d) % pn
        return remote(sb.at[b, q], ab.at[b, d], ps.at[b, d], pr.at[b, d], z * pn + q, t)

    def back(b, d):
        q = (p - d + pn) % pn
        return remote(ob.at[b, d], rb.at[b, p], rs.at[b, d], rr.at[b, d], z * pn + q, t)

    def home(b):
        return remote(pb.at[b], qb.at[z], cs.at[b], cr.at[z], b * pn + p, t)

    def arrived(b):
        remote(maps_ref.at[z], zm.at[b], ms.at[z], mr.at[b], b * pn + p, t).wait_recv()
        remote(normed_ref, zb.at[b], zs.at[b, 0], zr.at[b], b * pn + p, t).wait_recv()

    for dz in range(1, nz):
        maps_along(dz).start()

    @pl.when(z > 0)
    def _():
        hop(normed_ref, z, -1).start()

    @pl.when(z < nz - 1)
    def _():
        hop(normed_ref, z, 1).start()

    zb[z] = normed_ref[...]
    zm[z] = maps_ref[z]

    def pick(b):
        chosen = lax.dot_general(zm[b][:, :slots], zb[b], TN, preferred_element_type=F32)
        for q in range(pn):
            sb[b, q] = chosen[q * cap : (q + 1) * cap].astype(BF16)
        ab[b, 0] = sb[b, p]
        for d in range(1, pn):
            across(b, d).start()

    def take(b):
        arrived(b)

        @pl.when((b > z) & (z > 0))
        def _():
            hop(zb.at[b], b, -1).start()

        @pl.when((b < z) & (z < nz - 1))
        def _():
            hop(zb.at[b], b, 1).start()

        pick(b)

    pick(z)
    if nz > 1:
        take(near[1])
    for copy in loads:
        copy.wait()
    normed = normed_ref[...]
    shared_inner = (
        silu(jnp.dot(normed, sg[...], preferred_element_type=F32))
        * jnp.dot(normed, su[...], preferred_element_type=F32)
    ).astype(BF16)
    acc[...] = stream_ref[...].astype(F32) + jnp.dot(
        shared_inner, sd[...], preferred_element_type=F32
    )
    for k in range(2, nz):
        take(near[k])

    def turn_of(k):
        place = jnp.int32(0)
        for at in range(nz):
            place = place + jnp.where(k == at, near[(at + 1) % nz], 0)
        return place

    def stack(ref, dz):
        if cap % 16 == 0:
            return ref[dz].reshape(slots, width)
        return jnp.concatenate([ref[dz, d].astype(F32) for d in range(pn)], axis=0).astype(BF16)

    def expert(k, carried):
        b = turn_of(k)
        for d in range(1, pn):
            across(b, d).wait_recv()
        rows = stack(ab, b)
        halves = []
        for h in range(2):
            gate_act = jnp.dot(rows, wg[h], preferred_element_type=F32)
            up_act = jnp.dot(rows, wu[h], preferred_element_type=F32)
            inner = (silu(gate_act) * up_act).astype(BF16)
            halves.append(jnp.dot(inner, wd[h], preferred_element_type=F32).astype(BF16))
        summed = halves[0].astype(F32) + halves[1].astype(F32)
        for d in range(pn):
            ob[b, d] = summed[d * cap : (d + 1) * cap].astype(BF16)
        rb[b, p] = ob[b, 0]
        for d in range(1, pn):
            back(b, d).start()
        return carried

    lax.fori_loop(0, nz, expert, 0)

    def returned(b):
        for d in range(1, pn):
            back(b, d).wait_recv()
        return jnp.dot(zm[b][:, slots:], stack(rb, b), preferred_element_type=F32)

    def combine(k, carried):
        b = turn_of(k)
        pb[b] = returned(b).astype(BF16)
        home(b).start()
        return carried

    lax.fori_loop(0, nz - 1, combine, 0)
    total = acc[...] + returned(z)
    for k in range(1, nz):
        b = near[k]
        remote(pb.at[b], qb.at[b], cs.at[b], cr.at[b], b * pn + p, t).wait_recv()
        total = total + qb[b].astype(F32)
    out_ref[...] = total.astype(BF16)
    for dz in range(1, nz):
        maps_along(dz).wait_send()

    @pl.when(z > 0)
    def _():
        hop(normed_ref, z, -1).wait_send()

    @pl.when(z < nz - 1)
    def _():
        hop(normed_ref, z, 1).wait_send()

    for k in range(1, nz):
        b = near[k]
        home(b).wait_send()

        @pl.when((b > z) & (z > 0))
        def _():
            hop(zb.at[b], b, -1).wait_send()

        @pl.when((b < z) & (z < nz - 1))
        def _():
            hop(zb.at[b], b, 1).wait_send()

    for b in range(nz):
        for d in range(1, pn):
            across(b, d).wait_send()
            back(b, d).wait_send()


def experts(n, nz, cap, normed, stream, maps, weights, shared):
    pn = n // nz
    rows, width = normed.shape
    hidden = weights[0].shape[1]
    shared_hidden = shared[0].shape[1]
    anywhere = pl.BlockSpec(memory_space=pl.ANY)
    inside = pl.BlockSpec(memory_space=pltpu.VMEM)
    plane = (nz, pn, cap, width)
    dma = pltpu.SemaphoreType.DMA
    return pl.pallas_call(
        functools.partial(moe_kernel, n, nz, cap),
        out_shape=jax.ShapeDtypeStruct((rows, width), BF16),
        in_specs=[inside] * 3 + [anywhere] * 9,
        out_specs=inside,
        scratch_shapes=[
            pltpu.VMEM((2, width, hidden), BF16),
            pltpu.VMEM((2, width, hidden), BF16),
            pltpu.VMEM((2, hidden, width), BF16),
            pltpu.VMEM((width, shared_hidden), BF16),
            pltpu.VMEM((width, shared_hidden), BF16),
            pltpu.VMEM((shared_hidden, width), BF16),
            pltpu.VMEM((nz, rows, width), BF16),
            pltpu.VMEM((nz, rows, maps.shape[2]), BF16),
            pltpu.VMEM(plane, BF16),
            pltpu.VMEM(plane, BF16),
            pltpu.VMEM(plane, BF16),
            pltpu.VMEM(plane, BF16),
            pltpu.VMEM((nz, rows, width), BF16),
            pltpu.VMEM((nz, rows, width), BF16),
            pltpu.VMEM((rows, width), F32),
            dma((9,)),
            dma((nz, 2)), dma((nz,)), dma((nz,)), dma((nz,)),
            dma((nz, pn)), dma((nz, pn)), dma((nz, pn)), dma((nz, pn)),
            dma((nz,)), dma((nz,)),
        ],
        compiler_params=pltpu.CompilerParams(
            collective_id=1, has_side_effects=True, vmem_limit_bytes=60 * 1024 * 1024
        ),
        name="experts",
    )(normed, stream, maps, *weights, *shared)


def shards(
    n,
    stream_in,
    query_compressed,
    keyvalue_compressed,
    rope_key,
    query_norm_gain,
    keyvalue_norm_gain,
    query_up_weight,
    keyvalue_up_weight,
    out_proj,
    ffn_gain,
    expert_ids,
    expert_weights,
    expert_gate,
    expert_up,
    expert_down,
    shared_gate,
    shared_up,
    shared_down,
):
    nz = line_length(n)
    tok_rows = query_compressed.shape[0]
    head_width = KEY_PLAIN_WIDTH + ROTARY_WIDTH
    all_heads = query_up_weight.shape[1] // head_width
    local_heads = all_heads // 2
    sp_index = lax.axis_index("sp")
    tp_index = lax.axis_index("tp")
    own_pos = sp_index * tok_rows + jnp.arange(tok_rows, dtype=jnp.int32)
    cos_part, sine_part = turn_tables(own_pos, ROTARY_WIDTH)

    keyval_normed = rms_scale(keyvalue_compressed, keyvalue_norm_gain).astype(BF16)
    shared_rot = turn(rope_key.astype(F32), cos_part, sine_part).astype(BF16)
    fill = jnp.zeros((tok_rows, LANES - ROTARY_WIDTH), BF16)
    packed = jnp.concatenate([keyval_normed, shared_rot, fill], axis=1)
    kv, gate_other, up_other, down_other = gather_latents(
        n, nz, packed, expert_gate[0], expert_up[0], expert_down[0]
    )
    kv = kv.reshape(n * tok_rows, packed.shape[1])

    query_normed = rms_scale(query_compressed, query_norm_gain).astype(BF16)
    blank = jnp.zeros((tok_rows, LANES - ROTARY_WIDTH), F32)
    cos_table = jnp.concatenate([cos_part, cos_part, blank], axis=1)
    sin_table = jnp.concatenate([-sine_part, sine_part, blank], axis=1)
    local_out = attend(
        tp_index, query_normed, cos_table, sin_table, query_up_weight, keyvalue_up_weight, kv,
        local_heads,
    )

    attended = lax.all_to_all(local_out, "tp", split_axis=0, concat_axis=1, tiled=True)
    projected = jnp.dot(attended, out_proj, preferred_element_type=F32)
    stream = (stream_in.astype(F32) + projected).astype(BF16)
    normed = rms_scale(stream, ffn_gain).astype(BF16)

    shares = (
        routed_scale * expert_weights / jnp.sum(expert_weights, axis=-1, keepdims=True)
    ).astype(BF16)
    moe_rows = stream_in.shape[0]
    top_count = expert_ids.shape[1]
    expert_count = expert_gate.shape[0] * n
    capacity = 2 * moe_rows * top_count // expert_count
    slots = expert_count // nz * capacity
    flat_ids = expert_ids.reshape(-1)
    hot_ids = (flat_ids[:, None] == jnp.arange(expert_count, dtype=jnp.int32)[None, :]).astype(
        jnp.int32
    )
    rank_ids = jnp.sum((jnp.cumsum(hot_ids, axis=0) - hot_ids) * hot_ids, axis=1)
    slot_ids = flat_ids * capacity + rank_ids
    hot_slots = (
        slot_ids[:, None] == jnp.arange(expert_count * capacity, dtype=jnp.int32)[None, :]
    ).reshape(moe_rows, top_count, expert_count * capacity)
    sender_map = jnp.any(hot_slots, axis=1).astype(BF16).reshape(moe_rows, nz, slots)
    share_map = jnp.sum(
        jnp.where(hot_slots, shares[:, :, None], jnp.zeros((), BF16)), axis=1
    ).reshape(moe_rows, nz, slots)
    maps = jnp.transpose(jnp.concatenate([sender_map, share_map], axis=2), (1, 0, 2))
    return experts(
        n, nz, capacity, normed, stream, maps,
        (expert_gate[0], expert_up[0], expert_down[0], gate_other, up_other, down_other),
        (shared_gate, shared_up, shared_down),
    )


def solution(mesh):
    in_specs = (
        P(("sp", "tp"), None),
        P("sp", None),
        P("sp", None),
        P("sp", None),
        P(),
        P(),
        P(),
        P(),
        P(),
        P(),
        P(("sp", "tp"), None),
        P(("sp", "tp"), None),
        P("sp", None, "tp"),
        P("sp", None, "tp"),
        P("sp", "tp", None),
        P(),
        P(),
        P(),
    )
    return jax.shard_map(
        functools.partial(shards, mesh.shape["sp"]),
        mesh=mesh,
        in_specs=in_specs,
        out_specs=P(("sp", "tp"), None),
        check_vma=False,
    )
```

```python
import functools

import jax
import jax.numpy as jnp
from jax import lax
from jax.experimental import pallas as pl
from jax.experimental.pallas import tpu as pltpu
from jax.sharding import PartitionSpec as P

KEY_PLAIN_WIDTH = 128
ROTARY_WIDTH = 64
VALUE_HEAD_WIDTH = 128
LANES = 128

epsilon = 1e-06
routed_scale = 2.5
theta_base = 10000.0
MESH = pl.DeviceIdType.MESH
F32 = jnp.float32
BF16 = jnp.bfloat16


def rms_scale(values, scales):
    widened = values.astype(F32)
    inverse = lax.rsqrt(jnp.mean(widened * widened, axis=-1, keepdims=True) + epsilon)
    return widened * inverse * scales


def turn_tables(positions, rot_width):
    half_width = rot_width // 2
    frequency = theta_base ** (-(jnp.arange(half_width, dtype=F32) * 2.0) / rot_width)
    angles = positions.astype(F32)[:, None] * frequency[None, :]
    return (jnp.cos(angles), jnp.sin(angles))


def turn(values, cos_part, sine_part):
    lower_half, upper_half = jnp.split(values, 2, axis=-1)
    return jnp.concatenate(
        [
            lower_half * cos_part - upper_half * sine_part,
            upper_half * cos_part + lower_half * sine_part,
        ],
        axis=-1,
    )


def line_length(n):
    for candidate in (4, 2):
        if n % candidate == 0:
            return candidate
    return 1


def nearest(nz, z, k):
    place = jnp.int32(0)
    for at in range(nz):
        order = sorted(range(nz), key=lambda other: (abs(other - at), other))
        place = place + jnp.where(z == at, order[k], 0)
    return place


def remote(src, dst, send_sem, recv_sem, sp, tp):
    return pltpu.make_async_remote_copy(
        src_ref=src,
        dst_ref=dst,
        send_sem=send_sem,
        recv_sem=recv_sem,
        device_id=(sp, tp),
        device_id_type=MESH,
    )


def greet(n, nz, with_partner):
    pn = n // nz
    me, t = lax.axis_index("sp"), lax.axis_index("tp")
    z, p = me // pn, me % pn
    barrier = pltpu.get_barrier_semaphore()
    for dz in range(1, nz):
        pl.semaphore_signal(
            barrier, inc=1, device_id=(((z + dz) % nz) * pn + p, t), device_id_type=MESH
        )
    for d in range(1, pn):
        pl.semaphore_signal(
            barrier, inc=1, device_id=(z * pn + (p + d) % pn, t), device_id_type=MESH
        )
    if with_partner:
        pl.semaphore_signal(barrier, inc=1, device_id=(me, 1 - t), device_id_type=MESH)
    pl.semaphore_wait(barrier, nz - 1 + pn - 1 + (1 if with_partner else 0))


def gather_kernel(
    n, nz, x_ref, g_ref, u_ref, d_ref, kv_ref, go_ref, uo_ref, do_ref,
    zs, zr, ps, pr, xs, xr, ws, wr,
):
    pn = n // nz
    me, t = lax.axis_index("sp"), lax.axis_index("tp")
    z, p = me // pn, me % pn
    greet(n, nz, True)

    def block_of(dz, d):
        return ((z - dz + nz) % nz) * pn + (p - d + pn) % pn

    def along(dz):
        return remote(
            x_ref.at[t], kv_ref.at[me, t], zs.at[dz], zr.at[dz], ((z + dz) % nz) * pn + p, t
        )

    def across(dz, d):
        b = block_of(dz, 0)
        src = x_ref.at[t] if isinstance(dz, int) else kv_ref.at[b, t]
        return remote(
            src, kv_ref.at[b, t], ps.at[dz, d], pr.at[dz, d], z * pn + (p + d) % pn, t
        )

    def swap(dz, d):
        b = block_of(dz, d)
        return remote(
            kv_ref.at[b, t], kv_ref.at[b, t], xs.at[dz, d], xr.at[dz, d], me, 1 - t
        )

    weights = [
        remote(g_ref, go_ref, ws.at[0], wr.at[0], me, 1 - t),
        remote(u_ref, uo_ref, ws.at[1], wr.at[1], me, 1 - t),
        remote(d_ref, do_ref, ws.at[2], wr.at[2], me, 1 - t),
    ]
    away = [(nearest(nz, z, k) - z + nz) % nz for k in range(nz)]
    for k in range(1, nz):
        along(away[k]).start()
    for d in range(1, pn):
        across(0, d).start()
    for copy in weights:
        copy.start()
    kv_ref[me] = x_ref[...]
    behind = [jnp.int32(0)] + [(z - nearest(nz, z, k) + nz) % nz for k in range(1, nz)]
    for k in range(1, nz):
        dz = behind[k]
        along(dz).wait_recv()
        for d in range(1, pn):
            across(dz, d).start()
        swap(dz, 0).start()
    for k in range(nz):
        for d in range(1, pn):
            across(behind[k], d).wait_recv()
            swap(behind[k], d).start()
    for dz in range(nz):
        for d in range(pn):
            if dz or d:
                swap(dz, d).wait()
    for dz in range(1, nz):
        along(dz).wait_send()
    for dz in range(nz):
        for d in range(1, pn):
            across(dz, d).wait_send()
    for copy in weights:
        copy.wait()


def gather_latents(n, nz, packed, gate, up, down):
    pn = n // nz
    rows, width = packed.shape
    anywhere = pl.BlockSpec(memory_space=pl.ANY)
    inside = pl.BlockSpec(memory_space=pltpu.VMEM)
    return pl.pallas_call(
        functools.partial(gather_kernel, n, nz),
        out_shape=(
            jax.ShapeDtypeStruct((n, 2, rows // 2, width), BF16),
            jax.ShapeDtypeStruct(gate.shape, BF16),
            jax.ShapeDtypeStruct(up.shape, BF16),
            jax.ShapeDtypeStruct(down.shape, BF16),
        ),
        in_specs=[inside, anywhere, anywhere, anywhere],
        out_specs=(inside, anywhere, anywhere, anywhere),
        scratch_shapes=[
            pltpu.SemaphoreType.DMA((nz,)),
            pltpu.SemaphoreType.DMA((nz,)),
            pltpu.SemaphoreType.DMA((nz, pn)),
            pltpu.SemaphoreType.DMA((nz, pn)),
            pltpu.SemaphoreType.DMA((nz, pn)),
            pltpu.SemaphoreType.DMA((nz, pn)),
            pltpu.SemaphoreType.DMA((3,)),
            pltpu.SemaphoreType.DMA((3,)),
        ],
        compiler_params=pltpu.CompilerParams(collective_id=0, has_side_effects=True),
        name="gather_latents",
    )(packed.reshape(2, rows // 2, width), gate, up, down)


NT = (((1,), (1,)), ((), ()))
TN = (((0,), (0,)), ((), ()))


def attend_kernel(heads, t_ref, x_ref, cos_ref, sin_ref, wq_ref, w_ref, kv_ref, out_ref):
    latent = kv_ref.shape[1] - LANES
    pair = KEY_PLAIN_WIDTH + VALUE_HEAD_WIDTH
    rows = x_ref.shape[0]
    scale = (KEY_PLAIN_WIDTH + ROTARY_WIDTH) ** (-0.5)
    raw = jnp.dot(x_ref[...], wq_ref[...], preferred_element_type=F32) * scale
    first, middle, last = raw[:, :LANES], raw[:, LANES : 2 * LANES], raw[:, 2 * LANES :]
    lane = lax.broadcasted_iota(jnp.int32, (rows, LANES), 1)
    low = lane < ROTARY_WIDTH
    middle_swapped = pltpu.roll(middle, LANES - ROTARY_WIDTH, 1)
    last_swapped = pltpu.roll(last, LANES - ROTARY_WIDTH, 1)
    plain = (first, jnp.where(low, middle_swapped, last_swapped))
    half = ROTARY_WIDTH // 2
    parts = []
    for h, rotary in enumerate((middle, last_swapped)):
        other = jnp.where(
            lane < half, pltpu.roll(rotary, LANES - half, 1), pltpu.roll(rotary, half, 1)
        )
        turned = jnp.where(low, rotary * cos_ref[...] + other * sin_ref[...], 0.0).astype(BF16)
        wk = w_ref[:, h * pair : h * pair + KEY_PLAIN_WIDTH]
        qa = lax.dot_general(plain[h].astype(BF16), wk, NT, preferred_element_type=F32)
        parts.append(jnp.concatenate([qa.astype(BF16), turned], axis=1))
    q = jnp.concatenate(parts, axis=0)
    scores = lax.dot_general(q, kv_ref[...], NT, preferred_element_type=F32)
    weights = jnp.exp(scores - jnp.max(scores, axis=-1, keepdims=True))
    total = jnp.sum(weights, axis=-1, keepdims=True)
    mixed = jnp.dot(weights.astype(BF16), kv_ref[:, :latent], preferred_element_type=F32)
    mixed = (mixed / total).astype(BF16)
    for h in range(heads):
        wv = w_ref[:, h * pair + KEY_PLAIN_WIDTH : (h + 1) * pair]
        out_ref[:, h * VALUE_HEAD_WIDTH : (h + 1) * VALUE_HEAD_WIDTH] = jnp.dot(
            mixed[h * rows : (h + 1) * rows], wv, preferred_element_type=F32
        ).astype(BF16)


def attend(tp_index, query, cos_table, sin_table, query_weight, weight, kv, local_heads):
    heads = 2
    rows, rank = query.shape
    steps = local_heads // heads
    pair = KEY_PLAIN_WIDTH + VALUE_HEAD_WIDTH
    query_block = heads * (KEY_PLAIN_WIDTH + ROTARY_WIDTH)
    return pl.pallas_call(
        functools.partial(attend_kernel, heads),
        grid_spec=pltpu.PrefetchScalarGridSpec(
            num_scalar_prefetch=1,
            grid=(steps,),
            in_specs=[
                pl.BlockSpec((rows, rank), lambda i, t: (0, 0)),
                pl.BlockSpec((rows, LANES), lambda i, t: (0, 0)),
                pl.BlockSpec((rows, LANES), lambda i, t: (0, 0)),
                pl.BlockSpec((rank, query_block), lambda i, t: (0, t[0] * steps + i)),
                pl.BlockSpec((weight.shape[0], heads * pair), lambda i, t: (0, t[0] * steps + i)),
                pl.BlockSpec(kv.shape, lambda i, t: (0, 0)),
            ],
            out_specs=pl.BlockSpec((rows, heads * VALUE_HEAD_WIDTH), lambda i, t: (0, i)),
        ),
        out_shape=jax.ShapeDtypeStruct((rows, local_heads * VALUE_HEAD_WIDTH), BF16),
        compiler_params=pltpu.CompilerParams(vmem_limit_bytes=60 * 1024 * 1024),
        name="attend",
    )(tp_index.reshape(1), query, cos_table, sin_table, query_weight, weight, kv)


def silu(v):
    return v / (1.0 + jnp.exp(-v))


def moe_kernel(
    n, nz, cap,
    local_ref, stream_in_ref, gain_ref, maps_ref, g_ref, u_ref, d_ref, go_ref, uo_ref, do_ref,
    sg_ref, su_ref, sd_ref, proj_ref, out_ref,
    wg, wu, wd, sg, su, sd, proj, other, zb, zm, sb, ab, ob, rb, pb, qb, acc,
    ls, hs, hr, zs, zr, ms, mr, ps, pr, rs, rr, cs, cr,
):
    pn = n // nz
    slots = pn * cap
    width = stream_in_ref.shape[1]
    cols = local_ref.shape[2]
    me, t = lax.axis_index("sp"), lax.axis_index("tp")
    z, p = me // pn, me % pn
    mine = pl.ds(pl.multiple_of(t * cols, LANES), cols)
    theirs = pl.ds(pl.multiple_of((1 - t) * cols, LANES), cols)
    proj_loads = [
        pltpu.make_async_copy(proj_ref.at[part], proj.at[part], ls.at[9 + i])
        for i, part in enumerate((mine, theirs))
    ]
    for copy in proj_loads:
        copy.start()
    loads = [
        pltpu.make_async_copy(src, dst, ls.at[i])
        for i, (src, dst) in enumerate(
            [
                (g_ref, wg.at[0]), (go_ref, wg.at[1]), (u_ref, wu.at[0]), (uo_ref, wu.at[1]),
                (d_ref, wd.at[0]), (do_ref, wd.at[1]), (sg_ref, sg), (su_ref, su), (sd_ref, sd),
            ]
        )
    ]
    for copy in loads:
        copy.start()
    greet(n, nz, True)
    exchange = remote(local_ref.at[1 - t], other, hs.at[0], hr.at[0], me, 1 - t)
    exchange.start()

    near = [nearest(nz, z, k) for k in range(nz)]

    def hop(src, b, step):
        return remote(
            src, zb.at[b], zs.at[b, (step + 1) // 2], zr.at[b], (z + step) * pn + p, t
        )

    def maps_along(dz):
        to = (z + dz) % nz
        return remote(maps_ref.at[to], zm.at[z], ms.at[to], mr.at[z], to * pn + p, t)

    def across(b, d):
        q = (p + d) % pn
        return remote(sb.at[b, q], ab.at[b, d], ps.at[b, d], pr.at[b, d], z * pn + q, t)

    def back(b, d):
        q = (p - d + pn) % pn
        return remote(ob.at[b, d], rb.at[b, p], rs.at[b, d], rr.at[b, d], z * pn + q, t)

    def home(b):
        return remote(pb.at[b], qb.at[z], cs.at[b], cr.at[z], b * pn + p, t)

    def arrived(b):
        remote(maps_ref.at[z], zm.at[b], ms.at[z], mr.at[b], b * pn + p, t).wait_recv()
        remote(zb.at[b], zb.at[b], zs.at[b, 0], zr.at[b], b * pn + p, t).wait_recv()

    for dz in range(1, nz):
        maps_along(dz).start()
    zm[z] = maps_ref[z]
    proj_loads[0].wait()
    projected = jnp.dot(local_ref[t], proj[mine], preferred_element_type=F32)
    exchange.wait()
    proj_loads[1].wait()
    projected = projected + jnp.dot(other[...], proj[theirs], preferred_element_type=F32)
    stream = (stream_in_ref[...].astype(F32) + projected).astype(BF16).astype(F32)
    acc[...] = stream
    zb[z] = rms_scale(stream, gain_ref[...]).astype(BF16)

    @pl.when(z > 0)
    def _():
        hop(zb.at[z], z, -1).start()

    @pl.when(z < nz - 1)
    def _():
        hop(zb.at[z], z, 1).start()

    def pick(b):
        chosen = lax.dot_general(zm[b][:, :slots], zb[b], TN, preferred_element_type=F32)
        for q in range(pn):
            sb[b, q] = chosen[q * cap : (q + 1) * cap].astype(BF16)
        ab[b, 0] = sb[b, p]
        for d in range(1, pn):
            across(b, d).start()

    def take(b):
        arrived(b)

        @pl.when((b > z) & (z > 0))
        def _():
            hop(zb.at[b], b, -1).start()

        @pl.when((b < z) & (z < nz - 1))
        def _():
            hop(zb.at[b], b, 1).start()

        pick(b)

    pick(z)
    if nz > 1:
        take(near[1])
    for copy in loads:
        copy.wait()
    normed = zb[z]
    shared_inner = (
        silu(jnp.dot(normed, sg[...], preferred_element_type=F32))
        * jnp.dot(normed, su[...], preferred_element_type=F32)
    ).astype(BF16)
    acc[...] += jnp.dot(shared_inner, sd[...], preferred_element_type=F32)
    for k in range(2, nz):
        take(near[k])

    def turn_of(k):
        place = jnp.int32(0)
        for at in range(nz):
            place = place + jnp.where(k == at, near[(at + 1) % nz], 0)
        return place

    def stack(ref, dz):
        if cap % 16 == 0:
            return ref[dz].reshape(slots, width)
        return jnp.concatenate([ref[dz, d].astype(F32) for d in range(pn)], axis=0).astype(BF16)

    def expert(k, carried):
        b = turn_of(k)
        for d in range(1, pn):
            across(b, d).wait_recv()
        rows = stack(ab, b)
        halves = []
        for h in range(2):
            gate_act = jnp.dot(rows, wg[h], preferred_element_type=F32)
            up_act = jnp.dot(rows, wu[h], preferred_element_type=F32)
            inner = (silu(gate_act) * up_act).astype(BF16)
            halves.append(jnp.dot(inner, wd[h], preferred_element_type=F32).astype(BF16))
        summed = halves[0].astype(F32) + halves[1].astype(F32)
        for d in range(pn):
            ob[b, d] = summed[d * cap : (d + 1) * cap].astype(BF16)
        rb[b, p] = ob[b, 0]
        for d in range(1, pn):
            back(b, d).start()
        return carried

    lax.fori_loop(0, nz, expert, 0)

    def returned(b):
        for d in range(1, pn):
            back(b, d).wait_recv()
        return jnp.dot(zm[b][:, slots:], stack(rb, b), preferred_element_type=F32)

    def combine(k, carried):
        b = turn_of(k)
        pb[b] = returned(b).astype(BF16)
        home(b).start()
        return carried

    lax.fori_loop(0, nz - 1, combine, 0)
    total = acc[...] + returned(z)
    for k in range(1, nz):
        b = near[k]
        remote(pb.at[b], qb.at[b], cs.at[b], cr.at[b], b * pn + p, t).wait_recv()
        total = total + qb[b].astype(F32)
    out_ref[...] = total.astype(BF16)
    for dz in range(1, nz):
        maps_along(dz).wait_send()

    @pl.when(z > 0)
    def _():
        hop(zb.at[z], z, -1).wait_send()

    @pl.when(z < nz - 1)
    def _():
        hop(zb.at[z], z, 1).wait_send()

    for k in range(1, nz):
        b = near[k]
        home(b).wait_send()

        @pl.when((b > z) & (z > 0))
        def _():
            hop(zb.at[b], b, -1).wait_send()

        @pl.when((b < z) & (z < nz - 1))
        def _():
            hop(zb.at[b], b, 1).wait_send()

    for b in range(nz):
        for d in range(1, pn):
            across(b, d).wait_send()
            back(b, d).wait_send()


def experts(n, nz, cap, local_out, stream_in, gain, maps, weights, shared, out_proj):
    pn = n // nz
    rows, width = stream_in.shape
    cols = local_out.shape[1]
    hidden = weights[0].shape[1]
    shared_hidden = shared[0].shape[1]
    anywhere = pl.BlockSpec(memory_space=pl.ANY)
    inside = pl.BlockSpec(memory_space=pltpu.VMEM)
    plane = (nz, pn, cap, width)
    dma = pltpu.SemaphoreType.DMA
    return pl.pallas_call(
        functools.partial(moe_kernel, n, nz, cap),
        out_shape=jax.ShapeDtypeStruct((rows, width), BF16),
        in_specs=[inside] * 4 + [anywhere] * 10,
        out_specs=inside,
        scratch_shapes=[
            pltpu.VMEM((2, width, hidden), BF16),
            pltpu.VMEM((2, width, hidden), BF16),
            pltpu.VMEM((2, hidden, width), BF16),
            pltpu.VMEM((width, shared_hidden), BF16),
            pltpu.VMEM((width, shared_hidden), BF16),
            pltpu.VMEM((shared_hidden, width), BF16),
            pltpu.VMEM(out_proj.shape, BF16),
            pltpu.VMEM((rows, cols), BF16),
            pltpu.VMEM((nz, rows, width), BF16),
            pltpu.VMEM((nz, rows, maps.shape[2]), BF16),
            pltpu.VMEM(plane, BF16),
            pltpu.VMEM(plane, BF16),
            pltpu.VMEM(plane, BF16),
            pltpu.VMEM(plane, BF16),
            pltpu.VMEM((nz, rows, width), BF16),
            pltpu.VMEM((nz, rows, width), BF16),
            pltpu.VMEM((rows, width), F32),
            dma((11,)), dma((1,)), dma((1,)),
            dma((nz, 2)), dma((nz,)), dma((nz,)), dma((nz,)),
            dma((nz, pn)), dma((nz, pn)), dma((nz, pn)), dma((nz, pn)),
            dma((nz,)), dma((nz,)),
        ],
        compiler_params=pltpu.CompilerParams(
            collective_id=1, has_side_effects=True, vmem_limit_bytes=60 * 1024 * 1024
        ),
        name="experts",
    )(
        local_out.reshape(2, rows, cols), stream_in, gain.reshape(1, width), maps,
        *weights, *shared, out_proj,
    )


def shards(
    n,
    stream_in,
    query_compressed,
    keyvalue_compressed,
    rope_key,
    query_norm_gain,
    keyvalue_norm_gain,
    query_up_weight,
    keyvalue_up_weight,
    out_proj,
    ffn_gain,
    expert_ids,
    expert_weights,
    expert_gate,
    expert_up,
    expert_down,
    shared_gate,
    shared_up,
    shared_down,
):
    nz = line_length(n)
    tok_rows = query_compressed.shape[0]
    head_width = KEY_PLAIN_WIDTH + ROTARY_WIDTH
    all_heads = query_up_weight.shape[1] // head_width
    local_heads = all_heads // 2
    sp_index = lax.axis_index("sp")
    tp_index = lax.axis_index("tp")
    own_pos = sp_index * tok_rows + jnp.arange(tok_rows, dtype=jnp.int32)
    cos_part, sine_part = turn_tables(own_pos, ROTARY_WIDTH)

    keyval_normed = rms_scale(keyvalue_compressed, keyvalue_norm_gain).astype(BF16)
    shared_rot = turn(rope_key.astype(F32), cos_part, sine_part).astype(BF16)
    fill = jnp.zeros((tok_rows, LANES - ROTARY_WIDTH), BF16)
    packed = jnp.concatenate([keyval_normed, shared_rot, fill], axis=1)
    kv, gate_other, up_other, down_other = gather_latents(
        n, nz, packed, expert_gate[0], expert_up[0], expert_down[0]
    )
    kv = kv.reshape(n * tok_rows, packed.shape[1])

    query_normed = rms_scale(query_compressed, query_norm_gain).astype(BF16)
    blank = jnp.zeros((tok_rows, LANES - ROTARY_WIDTH), F32)
    cos_table = jnp.concatenate([cos_part, cos_part, blank], axis=1)
    sin_table = jnp.concatenate([-sine_part, sine_part, blank], axis=1)
    local_out = attend(
        tp_index, query_normed, cos_table, sin_table, query_up_weight, keyvalue_up_weight, kv,
        local_heads,
    )

    shares = (
        routed_scale * expert_weights / jnp.sum(expert_weights, axis=-1, keepdims=True)
    ).astype(BF16)
    moe_rows = stream_in.shape[0]
    top_count = expert_ids.shape[1]
    expert_count = expert_gate.shape[0] * n
    capacity = 2 * moe_rows * top_count // expert_count
    slots = expert_count // nz * capacity
    flat_ids = expert_ids.reshape(-1)
    hot_ids = (flat_ids[:, None] == jnp.arange(expert_count, dtype=jnp.int32)[None, :]).astype(
        jnp.int32
    )
    rank_ids = jnp.sum((jnp.cumsum(hot_ids, axis=0) - hot_ids) * hot_ids, axis=1)
    slot_ids = flat_ids * capacity + rank_ids
    hot_slots = (
        slot_ids[:, None] == jnp.arange(expert_count * capacity, dtype=jnp.int32)[None, :]
    ).reshape(moe_rows, top_count, expert_count * capacity)
    sender_map = jnp.any(hot_slots, axis=1).astype(BF16).reshape(moe_rows, nz, slots)
    share_map = jnp.sum(
        jnp.where(hot_slots, shares[:, :, None], jnp.zeros((), BF16)), axis=1
    ).reshape(moe_rows, nz, slots)
    maps = jnp.transpose(jnp.concatenate([sender_map, share_map], axis=2), (1, 0, 2))
    return experts(
        n, nz, capacity, local_out, stream_in, ffn_gain, maps,
        (expert_gate[0], expert_up[0], expert_down[0], gate_other, up_other, down_other),
        (shared_gate, shared_up, shared_down),
        out_proj,
    )


def solution(mesh):
    in_specs = (
        P(("sp", "tp"), None),
        P("sp", None),
        P("sp", None),
        P("sp", None),
        P(),
        P(),
        P(),
        P(),
        P(),
        P(),
        P(("sp", "tp"), None),
        P(("sp", "tp"), None),
        P("sp", None, "tp"),
        P("sp", None, "tp"),
        P("sp", "tp", None),
        P(),
        P(),
        P(),
    )
    return jax.shard_map(
        functools.partial(shards, mesh.shape["sp"]),
        mesh=mesh,
        in_specs=in_specs,
        out_specs=P(("sp", "tp"), None),
        check_vma=False,
    )
```

```python
import functools

import jax
import jax.numpy as jnp
from jax import lax
from jax.experimental import pallas as pl
from jax.experimental.pallas import tpu as pltpu
from jax.sharding import PartitionSpec as P

KEY_PLAIN_WIDTH = 128
ROTARY_WIDTH = 64
VALUE_HEAD_WIDTH = 128
LANES = 128

epsilon = 1e-06
routed_scale = 2.5
theta_base = 10000.0
MESH = pl.DeviceIdType.MESH
F32 = jnp.float32
BF16 = jnp.bfloat16


def rms_scale(values, scales):
    widened = values.astype(F32)
    inverse = lax.rsqrt(jnp.mean(widened * widened, axis=-1, keepdims=True) + epsilon)
    return widened * inverse * scales


def turn_tables(positions, rot_width):
    half_width = rot_width // 2
    frequency = theta_base ** (-(jnp.arange(half_width, dtype=F32) * 2.0) / rot_width)
    angles = positions.astype(F32)[:, None] * frequency[None, :]
    return (jnp.cos(angles), jnp.sin(angles))


def turn(values, cos_part, sine_part):
    lower_half, upper_half = jnp.split(values, 2, axis=-1)
    return jnp.concatenate(
        [
            lower_half * cos_part - upper_half * sine_part,
            upper_half * cos_part + lower_half * sine_part,
        ],
        axis=-1,
    )


def line_length(n):
    for candidate in (4, 2):
        if n % candidate == 0:
            return candidate
    return 1


def nearest(nz, z, k):
    place = jnp.int32(0)
    for at in range(nz):
        order = sorted(range(nz), key=lambda other: (abs(other - at), other))
        place = place + jnp.where(z == at, order[k], 0)
    return place


def remote(src, dst, send_sem, recv_sem, sp, tp):
    return pltpu.make_async_remote_copy(
        src_ref=src,
        dst_ref=dst,
        send_sem=send_sem,
        recv_sem=recv_sem,
        device_id=(sp, tp),
        device_id_type=MESH,
    )


def greet(n, nz, with_partner):
    pn = n // nz
    me, t = lax.axis_index("sp"), lax.axis_index("tp")
    z, p = me // pn, me % pn
    barrier = pltpu.get_barrier_semaphore()
    for dz in range(1, nz):
        pl.semaphore_signal(
            barrier, inc=1, device_id=(((z + dz) % nz) * pn + p, t), device_id_type=MESH
        )
    for d in range(1, pn):
        pl.semaphore_signal(
            barrier, inc=1, device_id=(z * pn + (p + d) % pn, t), device_id_type=MESH
        )
    if with_partner:
        pl.semaphore_signal(barrier, inc=1, device_id=(me, 1 - t), device_id_type=MESH)
    pl.semaphore_wait(barrier, nz - 1 + pn - 1 + (1 if with_partner else 0))


def gather_kernel(
    n, nz, x_ref, g_ref, u_ref, d_ref, kv_ref, go_ref, uo_ref, do_ref,
    zs, zr, ps, pr, xs, xr, ws, wr,
):
    pn = n // nz
    me, t = lax.axis_index("sp"), lax.axis_index("tp")
    z, p = me // pn, me % pn
    greet(n, nz, True)

    def block_of(dz, d):
        return ((z - dz + nz) % nz) * pn + (p - d + pn) % pn

    def along(dz):
        return remote(
            x_ref.at[t], kv_ref.at[me, t], zs.at[dz], zr.at[dz], ((z + dz) % nz) * pn + p, t
        )

    def across(dz, d):
        b = block_of(dz, 0)
        src = x_ref.at[t] if isinstance(dz, int) else kv_ref.at[b, t]
        return remote(
            src, kv_ref.at[b, t], ps.at[dz, d], pr.at[dz, d], z * pn + (p + d) % pn, t
        )

    def swap(dz, d):
        b = block_of(dz, d)
        return remote(
            kv_ref.at[b, t], kv_ref.at[b, t], xs.at[dz, d], xr.at[dz, d], me, 1 - t
        )

    weights = [
        remote(g_ref, go_ref, ws.at[0], wr.at[0], me, 1 - t),
        remote(u_ref, uo_ref, ws.at[1], wr.at[1], me, 1 - t),
        remote(d_ref, do_ref, ws.at[2], wr.at[2], me, 1 - t),
    ]
    away = [(nearest(nz, z, k) - z + nz) % nz for k in range(nz)]
    for k in range(1, nz):
        along(away[k]).start()
    for d in range(1, pn):
        across(0, d).start()
    for copy in weights:
        copy.start()
    kv_ref[me] = x_ref[...]
    behind = [jnp.int32(0)] + [(z - nearest(nz, z, k) + nz) % nz for k in range(1, nz)]
    for k in range(1, nz):
        dz = behind[k]
        along(dz).wait_recv()
        for d in range(1, pn):
            across(dz, d).start()
        swap(dz, 0).start()
    for k in range(nz):
        for d in range(1, pn):
            across(behind[k], d).wait_recv()
            swap(behind[k], d).start()
    for dz in range(nz):
        for d in range(pn):
            if dz or d:
                swap(dz, d).wait()
    for dz in range(1, nz):
        along(dz).wait_send()
    for dz in range(nz):
        for d in range(1, pn):
            across(dz, d).wait_send()
    for copy in weights:
        copy.wait()


def gather_latents(n, nz, packed, gate, up, down):
    pn = n // nz
    rows, width = packed.shape
    anywhere = pl.BlockSpec(memory_space=pl.ANY)
    inside = pl.BlockSpec(memory_space=pltpu.VMEM)
    return pl.pallas_call(
        functools.partial(gather_kernel, n, nz),
        out_shape=(
            jax.ShapeDtypeStruct((n, 2, rows // 2, width), BF16),
            jax.ShapeDtypeStruct(gate.shape, BF16),
            jax.ShapeDtypeStruct(up.shape, BF16),
            jax.ShapeDtypeStruct(down.shape, BF16),
        ),
        in_specs=[inside, anywhere, anywhere, anywhere],
        out_specs=(inside, anywhere, anywhere, anywhere),
        scratch_shapes=[
            pltpu.SemaphoreType.DMA((nz,)),
            pltpu.SemaphoreType.DMA((nz,)),
            pltpu.SemaphoreType.DMA((nz, pn)),
            pltpu.SemaphoreType.DMA((nz, pn)),
            pltpu.SemaphoreType.DMA((nz, pn)),
            pltpu.SemaphoreType.DMA((nz, pn)),
            pltpu.SemaphoreType.DMA((3,)),
            pltpu.SemaphoreType.DMA((3,)),
        ],
        compiler_params=pltpu.CompilerParams(collective_id=0, has_side_effects=True),
        name="gather_latents",
    )(packed.reshape(2, rows // 2, width), gate, up, down)


NT = (((1,), (1,)), ((), ()))
TN = (((0,), (0,)), ((), ()))


def attend_kernel(heads, t_ref, x_ref, cos_ref, sin_ref, wq_ref, w_ref, kv_ref, out_ref):
    latent = kv_ref.shape[1] - LANES
    pair = KEY_PLAIN_WIDTH + VALUE_HEAD_WIDTH
    rows = x_ref.shape[0]
    scale = (KEY_PLAIN_WIDTH + ROTARY_WIDTH) ** (-0.5)
    raw = jnp.dot(x_ref[...], wq_ref[...], preferred_element_type=F32) * scale
    first, middle, last = raw[:, :LANES], raw[:, LANES : 2 * LANES], raw[:, 2 * LANES :]
    lane = lax.broadcasted_iota(jnp.int32, (rows, LANES), 1)
    low = lane < ROTARY_WIDTH
    middle_swapped = pltpu.roll(middle, LANES - ROTARY_WIDTH, 1)
    last_swapped = pltpu.roll(last, LANES - ROTARY_WIDTH, 1)
    plain = (first, jnp.where(low, middle_swapped, last_swapped))
    half = ROTARY_WIDTH // 2
    parts = []
    for h, rotary in enumerate((middle, last_swapped)):
        other = jnp.where(
            lane < half, pltpu.roll(rotary, LANES - half, 1), pltpu.roll(rotary, half, 1)
        )
        turned = jnp.where(low, rotary * cos_ref[...] + other * sin_ref[...], 0.0).astype(BF16)
        wk = w_ref[:, h * pair : h * pair + KEY_PLAIN_WIDTH]
        qa = lax.dot_general(plain[h].astype(BF16), wk, NT, preferred_element_type=F32)
        parts.append(jnp.concatenate([qa.astype(BF16), turned], axis=1))
    q = jnp.concatenate(parts, axis=0)
    scores = lax.dot_general(q, kv_ref[...], NT, preferred_element_type=F32)
    weights = jnp.exp(scores - jnp.max(scores, axis=-1, keepdims=True))
    total = jnp.sum(weights, axis=-1, keepdims=True)
    mixed = jnp.dot(weights.astype(BF16), kv_ref[:, :latent], preferred_element_type=F32)
    mixed = (mixed / total).astype(BF16)
    for h in range(heads):
        wv = w_ref[:, h * pair + KEY_PLAIN_WIDTH : (h + 1) * pair]
        out_ref[:, h * VALUE_HEAD_WIDTH : (h + 1) * VALUE_HEAD_WIDTH] = jnp.dot(
            mixed[h * rows : (h + 1) * rows], wv, preferred_element_type=F32
        ).astype(BF16)


def attend(tp_index, query, cos_table, sin_table, query_weight, weight, kv, local_heads):
    heads = 2
    rows, rank = query.shape
    steps = local_heads // heads
    pair = KEY_PLAIN_WIDTH + VALUE_HEAD_WIDTH
    query_block = heads * (KEY_PLAIN_WIDTH + ROTARY_WIDTH)
    return pl.pallas_call(
        functools.partial(attend_kernel, heads),
        grid_spec=pltpu.PrefetchScalarGridSpec(
            num_scalar_prefetch=1,
            grid=(steps,),
            in_specs=[
                pl.BlockSpec((rows, rank), lambda i, t: (0, 0)),
                pl.BlockSpec((rows, LANES), lambda i, t: (0, 0)),
                pl.BlockSpec((rows, LANES), lambda i, t: (0, 0)),
                pl.BlockSpec((rank, query_block), lambda i, t: (0, t[0] * steps + i)),
                pl.BlockSpec((weight.shape[0], heads * pair), lambda i, t: (0, t[0] * steps + i)),
                pl.BlockSpec(kv.shape, lambda i, t: (0, 0)),
            ],
            out_specs=pl.BlockSpec((rows, heads * VALUE_HEAD_WIDTH), lambda i, t: (0, i)),
        ),
        out_shape=jax.ShapeDtypeStruct((rows, local_heads * VALUE_HEAD_WIDTH), BF16),
        compiler_params=pltpu.CompilerParams(vmem_limit_bytes=60 * 1024 * 1024),
        name="attend",
    )(tp_index.reshape(1), query, cos_table, sin_table, query_weight, weight, kv)


def silu(v):
    return v / (1.0 + jnp.exp(-v))


def moe_kernel(
    n, nz, cap,
    local_ref, stream_in_ref, gain_ref, maps_ref, g_ref, u_ref, d_ref, go_ref, uo_ref, do_ref,
    sg_ref, su_ref, sd_ref, proj_ref, out_ref,
    wg, wu, wd, sg, su, sd, proj, other, zb, zm, sb, ab, ob, rb, pb, qb, acc,
    ls, hs, hr, zs, zr, ms, mr, ps, pr, rs, rr, cs, cr,
):
    pn = n // nz
    slots = pn * cap
    width = stream_in_ref.shape[1]
    cols = local_ref.shape[2]
    me, t = lax.axis_index("sp"), lax.axis_index("tp")
    z, p = me // pn, me % pn
    mine = pl.ds(pl.multiple_of(t * cols, LANES), cols)
    theirs = pl.ds(pl.multiple_of((1 - t) * cols, LANES), cols)
    proj_loads = [
        pltpu.make_async_copy(proj_ref.at[part], proj.at[part], ls.at[9 + i])
        for i, part in enumerate((mine, theirs))
    ]
    for copy in proj_loads:
        copy.start()
    loads = [
        pltpu.make_async_copy(src, dst, ls.at[i])
        for i, (src, dst) in enumerate(
            [
                (g_ref, wg.at[0]), (go_ref, wg.at[1]), (u_ref, wu.at[0]), (uo_ref, wu.at[1]),
                (d_ref, wd.at[0]), (do_ref, wd.at[1]), (sg_ref, sg), (su_ref, su), (sd_ref, sd),
            ]
        )
    ]
    for copy in loads:
        copy.start()
    greet(n, nz, True)
    exchange = remote(local_ref.at[1 - t], other, hs.at[0], hr.at[0], me, 1 - t)
    exchange.start()

    near = [nearest(nz, z, k) for k in range(nz)]

    def hop(src, b, step):
        return remote(
            src, zb.at[b], zs.at[b, (step + 1) // 2], zr.at[b], (z + step) * pn + p, t
        )

    def maps_along(dz):
        to = (z + dz) % nz
        return remote(maps_ref.at[to], zm.at[z], ms.at[to], mr.at[z], to * pn + p, t)

    def across(b, d):
        q = (p + d) % pn
        return remote(sb.at[b, q], ab.at[b, d], ps.at[b, d], pr.at[b, d], z * pn + q, t)

    def back(b, d):
        q = (p - d + pn) % pn
        return remote(ob.at[b, d], rb.at[b, p], rs.at[b, d], rr.at[b, d], z * pn + q, t)

    def home(b):
        return remote(pb.at[b], qb.at[z], cs.at[b], cr.at[z], b * pn + p, t)

    def arrived(b):
        remote(maps_ref.at[z], zm.at[b], ms.at[z], mr.at[b], b * pn + p, t).wait_recv()
        remote(zb.at[b], zb.at[b], zs.at[b, 0], zr.at[b], b * pn + p, t).wait_recv()

    for dz in range(1, nz):
        maps_along(dz).start()
    zm[z] = maps_ref[z]
    proj_loads[0].wait()
    projected = jnp.dot(local_ref[t], proj[mine], preferred_element_type=F32)
    exchange.wait()
    proj_loads[1].wait()
    projected = projected + jnp.dot(other[...], proj[theirs], preferred_element_type=F32)
    stream = (stream_in_ref[...].astype(F32) + projected).astype(BF16).astype(F32)
    acc[...] = stream
    zb[z] = rms_scale(stream, gain_ref[...]).astype(BF16)

    @pl.when(z > 0)
    def _():
        hop(zb.at[z], z, -1).start()

    @pl.when(z < nz - 1)
    def _():
        hop(zb.at[z], z, 1).start()

    def pick(b):
        chosen = lax.dot_general(zm[b][:, :slots], zb[b], TN, preferred_element_type=F32)
        for q in range(pn):
            sb[b, q] = chosen[q * cap : (q + 1) * cap].astype(BF16)
        ab[b, 0] = sb[b, p]
        for d in range(1, pn):
            across(b, d).start()

    def take(b):
        arrived(b)

        @pl.when((b > z) & (z > 0))
        def _():
            hop(zb.at[b], b, -1).start()

        @pl.when((b < z) & (z < nz - 1))
        def _():
            hop(zb.at[b], b, 1).start()

        pick(b)

    pick(z)
    if nz > 1:
        take(near[1])
    for copy in loads:
        copy.wait()
    normed = zb[z]
    shared_inner = (
        silu(jnp.dot(normed, sg[...], preferred_element_type=F32))
        * jnp.dot(normed, su[...], preferred_element_type=F32)
    ).astype(BF16)
    acc[...] += jnp.dot(shared_inner, sd[...], preferred_element_type=F32)
    def turn_of(k):
        place = jnp.int32(0)
        for at in range(nz):
            place = place + jnp.where(k == at, near[(at + 1) % nz], 0)
        return place

    def stack(ref, dz):
        if cap % 16 == 0:
            return ref[dz].reshape(slots, width)
        return jnp.concatenate([ref[dz, d].astype(F32) for d in range(pn)], axis=0).astype(BF16)

    def expert(b):
        for d in range(1, pn):
            across(b, d).wait_recv()
        rows = stack(ab, b)
        halves = []
        for h in range(2):
            gate_act = jnp.dot(rows, wg[h], preferred_element_type=F32)
            up_act = jnp.dot(rows, wu[h], preferred_element_type=F32)
            inner = (silu(gate_act) * up_act).astype(BF16)
            halves.append(jnp.dot(inner, wd[h], preferred_element_type=F32).astype(BF16))
        summed = halves[0].astype(F32) + halves[1].astype(F32)
        for d in range(pn):
            ob[b, d] = summed[d * cap : (d + 1) * cap].astype(BF16)
        rb[b, p] = ob[b, 0]

    def give(b):
        for d in range(1, pn):
            back(b, d).start()

    expert(z)
    for k in range(2, nz):
        if k > 2:
            expert(near[k - 2])
        take(near[k])
    for k in range(1, nz):
        if k > max(nz - 3, 0):
            expert(near[k])
        give(near[k])
    give(z)

    def returned(b):
        for d in range(1, pn):
            back(b, d).wait_recv()
        return jnp.dot(zm[b][:, slots:], stack(rb, b), preferred_element_type=F32)

    def combine(k, carried):
        b = turn_of(k)
        pb[b] = returned(b).astype(BF16)
        home(b).start()
        return carried

    lax.fori_loop(0, nz - 1, combine, 0)
    total = acc[...] + returned(z)
    for k in range(1, nz):
        b = near[k]
        remote(pb.at[b], qb.at[b], cs.at[b], cr.at[b], b * pn + p, t).wait_recv()
        total = total + qb[b].astype(F32)
    out_ref[...] = total.astype(BF16)
    for dz in range(1, nz):
        maps_along(dz).wait_send()

    @pl.when(z > 0)
    def _():
        hop(zb.at[z], z, -1).wait_send()

    @pl.when(z < nz - 1)
    def _():
        hop(zb.at[z], z, 1).wait_send()

    for k in range(1, nz):
        b = near[k]
        home(b).wait_send()

        @pl.when((b > z) & (z > 0))
        def _():
            hop(zb.at[b], b, -1).wait_send()

        @pl.when((b < z) & (z < nz - 1))
        def _():
            hop(zb.at[b], b, 1).wait_send()

    for b in range(nz):
        for d in range(1, pn):
            across(b, d).wait_send()
            back(b, d).wait_send()


def experts(n, nz, cap, local_out, stream_in, gain, maps, weights, shared, out_proj):
    pn = n // nz
    rows, width = stream_in.shape
    cols = local_out.shape[1]
    hidden = weights[0].shape[1]
    shared_hidden = shared[0].shape[1]
    anywhere = pl.BlockSpec(memory_space=pl.ANY)
    inside = pl.BlockSpec(memory_space=pltpu.VMEM)
    plane = (nz, pn, cap, width)
    dma = pltpu.SemaphoreType.DMA
    return pl.pallas_call(
        functools.partial(moe_kernel, n, nz, cap),
        out_shape=jax.ShapeDtypeStruct((rows, width), BF16),
        in_specs=[inside] * 4 + [anywhere] * 10,
        out_specs=inside,
        scratch_shapes=[
            pltpu.VMEM((2, width, hidden), BF16),
            pltpu.VMEM((2, width, hidden), BF16),
            pltpu.VMEM((2, hidden, width), BF16),
            pltpu.VMEM((width, shared_hidden), BF16),
            pltpu.VMEM((width, shared_hidden), BF16),
            pltpu.VMEM((shared_hidden, width), BF16),
            pltpu.VMEM(out_proj.shape, BF16),
            pltpu.VMEM((rows, cols), BF16),
            pltpu.VMEM((nz, rows, width), BF16),
            pltpu.VMEM((nz, rows, maps.shape[2]), BF16),
            pltpu.VMEM(plane, BF16),
            pltpu.VMEM(plane, BF16),
            pltpu.VMEM(plane, BF16),
            pltpu.VMEM(plane, BF16),
            pltpu.VMEM((nz, rows, width), BF16),
            pltpu.VMEM((nz, rows, width), BF16),
            pltpu.VMEM((rows, width), F32),
            dma((11,)), dma((1,)), dma((1,)),
            dma((nz, 2)), dma((nz,)), dma((nz,)), dma((nz,)),
            dma((nz, pn)), dma((nz, pn)), dma((nz, pn)), dma((nz, pn)),
            dma((nz,)), dma((nz,)),
        ],
        compiler_params=pltpu.CompilerParams(
            collective_id=1, has_side_effects=True, vmem_limit_bytes=60 * 1024 * 1024
        ),
        name="experts",
    )(
        local_out.reshape(2, rows, cols), stream_in, gain.reshape(1, width), maps,
        *weights, *shared, out_proj,
    )


def shards(
    n,
    stream_in,
    query_compressed,
    keyvalue_compressed,
    rope_key,
    query_norm_gain,
    keyvalue_norm_gain,
    query_up_weight,
    keyvalue_up_weight,
    out_proj,
    ffn_gain,
    expert_ids,
    expert_weights,
    expert_gate,
    expert_up,
    expert_down,
    shared_gate,
    shared_up,
    shared_down,
):
    nz = line_length(n)
    tok_rows = query_compressed.shape[0]
    head_width = KEY_PLAIN_WIDTH + ROTARY_WIDTH
    all_heads = query_up_weight.shape[1] // head_width
    local_heads = all_heads // 2
    sp_index = lax.axis_index("sp")
    tp_index = lax.axis_index("tp")
    own_pos = sp_index * tok_rows + jnp.arange(tok_rows, dtype=jnp.int32)
    cos_part, sine_part = turn_tables(own_pos, ROTARY_WIDTH)

    keyval_normed = rms_scale(keyvalue_compressed, keyvalue_norm_gain).astype(BF16)
    shared_rot = turn(rope_key.astype(F32), cos_part, sine_part).astype(BF16)
    fill = jnp.zeros((tok_rows, LANES - ROTARY_WIDTH), BF16)
    packed = jnp.concatenate([keyval_normed, shared_rot, fill], axis=1)
    kv, gate_other, up_other, down_other = gather_latents(
        n, nz, packed, expert_gate[0], expert_up[0], expert_down[0]
    )
    kv = kv.reshape(n * tok_rows, packed.shape[1])

    query_normed = rms_scale(query_compressed, query_norm_gain).astype(BF16)
    blank = jnp.zeros((tok_rows, LANES - ROTARY_WIDTH), F32)
    cos_table = jnp.concatenate([cos_part, cos_part, blank], axis=1)
    sin_table = jnp.concatenate([-sine_part, sine_part, blank], axis=1)
    local_out = attend(
        tp_index, query_normed, cos_table, sin_table, query_up_weight, keyvalue_up_weight, kv,
        local_heads,
    )

    shares = (
        routed_scale * expert_weights / jnp.sum(expert_weights, axis=-1, keepdims=True)
    ).astype(BF16)
    moe_rows = stream_in.shape[0]
    top_count = expert_ids.shape[1]
    expert_count = expert_gate.shape[0] * n
    capacity = 2 * moe_rows * top_count // expert_count
    slots = expert_count // nz * capacity
    flat_ids = expert_ids.reshape(-1)
    hot_ids = (flat_ids[:, None] == jnp.arange(expert_count, dtype=jnp.int32)[None, :]).astype(
        jnp.int32
    )
    rank_ids = jnp.sum((jnp.cumsum(hot_ids, axis=0) - hot_ids) * hot_ids, axis=1)
    slot_ids = flat_ids * capacity + rank_ids
    hot_slots = (
        slot_ids[:, None] == jnp.arange(expert_count * capacity, dtype=jnp.int32)[None, :]
    ).reshape(moe_rows, top_count, expert_count * capacity)
    sender_map = jnp.any(hot_slots, axis=1).astype(BF16).reshape(moe_rows, nz, slots)
    share_map = jnp.sum(
        jnp.where(hot_slots, shares[:, :, None], jnp.zeros((), BF16)), axis=1
    ).reshape(moe_rows, nz, slots)
    maps = jnp.transpose(jnp.concatenate([sender_map, share_map], axis=2), (1, 0, 2))
    return experts(
        n, nz, capacity, local_out, stream_in, ffn_gain, maps,
        (expert_gate[0], expert_up[0], expert_down[0], gate_other, up_other, down_other),
        (shared_gate, shared_up, shared_down),
        out_proj,
    )


def solution(mesh):
    in_specs = (
        P(("sp", "tp"), None),
        P("sp", None),
        P("sp", None),
        P("sp", None),
        P(),
        P(),
        P(),
        P(),
        P(),
        P(),
        P(("sp", "tp"), None),
        P(("sp", "tp"), None),
        P("sp", None, "tp"),
        P("sp", None, "tp"),
        P("sp", "tp", None),
        P(),
        P(),
        P(),
    )
    return jax.shard_map(
        functools.partial(shards, mesh.shape["sp"]),
        mesh=mesh,
        in_specs=in_specs,
        out_specs=P(("sp", "tp"), None),
        check_vma=False,
    )
```
